32 devices in a mesh: tp: 8 (over z, y), dp: 4 (over x, core).
Axes of the slice: x: 2, y: 2, z: 4, core: 2. Of those that a mesh axis runs over, the one named last changes fastest.
Arguments:
- tokens: bfloat16 [32, 16, 4096], P('tp', None, 'dp'), may hold values from -24 to 24
- lengths: int32 [32], P('dp'), may hold values from 1 to 16, 224 in all
- norm_gain: float32 [2, 4096], P(None, 'dp'), may hold values from 0.1 to 1.9
- query_weight: bfloat16 [2, 4096, 4096], P(None, 'dp', 'tp'), may hold values from -0.09375 to 0.09375
- key_weight: bfloat16 [2, 4096, 4096], P(None, 'dp', 'tp'), may hold values from -0.09375 to 0.09375
- value_weight: bfloat16 [2, 4096, 4096], P(None, 'dp', 'tp'), may hold values from -0.09375 to 0.09375
- outgate_weight: bfloat16 [2, 4096, 4096], P(None, 'dp', 'tp'), may hold values from -0.09375 to 0.09375
- input_gate_weight: bfloat16 [2, 4096, 32], replicated, may hold values from -0.09375 to 0.09375
- forget_gate_weight: bfloat16 [2, 4096, 32], replicated, may hold values from -0.09375 to 0.09375
- forget_bias: float32 [2, 32], P(None, 'tp'), may hold values from -1 to 6
- out_weight: bfloat16 [2, 4096, 4096], P(None, 'tp', 'dp'), may hold values from -0.09375 to 0.09375
- cell_state: float32 [2, 32, 32, 128, 128], P(None, 'dp', 'tp'), may hold values from -1.5 to 1.5
- norm_state: float32 [2, 32, 32, 128], P(None, 'dp', 'tp'), may hold values from -1.5 to 1.5
- max_state: float32 [2, 32, 32], P(None, 'dp', 'tp'), may hold values from -6 to 6
Outputs:
- tokens_next: bfloat16 [32, 16, 4096], P('tp', None, 'dp')
- cell_next: float32 [2, 32, 32, 128, 128], P(None, 'dp', 'tp')
- norm_next: float32 [2, 32, 32, 128], P(None, 'dp', 'tp')
- max_next: float32 [2, 32, 32], P(None, 'dp', 'tp')
The draws below stay inside these ranges and needn't reach their ends.
Inputs may be any that keep to these rules, and one draw needn't show every extreme that they name: `lengths`: the largest is 16.
All inputs are finite; a program needn't handle non-finite values. No bound on the sum of `lengths` on one device may be relied on, other than what follows from the above.
Results may differ from the reference program's by a relative error of at most 0.025.
Values may be sent and summed in bfloat16 or wider, within the bound.
A program may use at most 64 MiB of HBM per device.

```python
import math
import jax
import jax.numpy as jnp
import numpy as np
from jax import lax

D = 4096
HEADS = 32
HEAD_DIM = 128
STEP = 16
SEQS = 32
W = 4096
N_DP = 4


def draw_tokens(key, part):
    first = jax.random.fold_in(jax.random.fold_in(key, 11), 0)
    position = jnp.arange(D, dtype=jnp.float32) / D
    noise = jnp.clip(jax.random.normal(first, (SEQS, STEP, D), jnp.float32), -4.0, 4.0)
    ramp_scale = 0.5 * jnp.exp(jnp.log(4.0) * position)
    return (noise * ramp_scale).astype(jnp.bfloat16)


def shard_levels(stream_key, shape, shards, low, high):
    def one(axis_at, parts):
        draws = jax.random.uniform(jax.random.fold_in(jax.random.fold_in(stream_key, 6), axis_at), (parts,), jnp.float32, low / len(shards), high / len(shards))
        return jnp.repeat(jnp.exp(draws), shape[axis_at] // parts).reshape((-1,) + (1,) * (len(shape) - axis_at - 1))

    level = one(*shards[0])
    for cut in shards[1:]:
        level = level * one(*cut)
    return level


def profile(count, total, most, skew):
    loads = [(1 << 20) // math.isqrt(standing ** skew) + 1 for standing in range(2, count + 1)]
    surplus, holding = total - most - (count - 1), [1] * (count - 1)
    while surplus > 0:
        candidates = [i for i in range(count - 1) if holding[i] < most]
        whole, remaining = sum([loads[i] for i in candidates]), surplus
        for i in candidates:
            extra = min(most - holding[i], max(1, remaining * loads[i] // whole), surplus)
            holding[i] = holding[i] + extra
            surplus = surplus - extra
    return np.array([most] + holding)


def ragged_sizes(stream_key, count, total, reach, slope):
    if count == 2:
        one = jax.random.randint(stream_key, (), max(1, total - reach), min(reach, total - 1) + 1)
        return jnp.stack([one, total - one])
    sizes = jnp.asarray(profile(count, total, reach, slope), jnp.int32)
    twos = (count - 1) // 2
    donor, taker = sizes[1:1 + 2 * twos:2], sizes[2:2 + 2 * twos:2]
    margin = jnp.minimum(donor - 1, reach - taker)
    passed = jax.random.randint(jax.random.fold_in(stream_key, 1), (twos,), 0, 1 << 20) % (margin + 1)
    sizes = sizes.at[1:1 + 2 * twos:2].set(donor - passed).at[2:2 + 2 * twos:2].set(taker + passed)
    return sizes[jax.random.permutation(jax.random.fold_in(stream_key, 2), count)]


def bell_draw(stream_key, extent, scale, reach, cuts=(), kind=jnp.bfloat16):
    array = scale * jax.random.normal(stream_key, extent, jnp.float32)
    if cuts:
        array = array * shard_levels(stream_key, extent, cuts, -0.22, 0.18)
    return jnp.clip(array, -reach, reach).astype(kind)


def setup_inputs(seed: int = 0) -> dict:
    key_of = jax.random.split(jax.random.key(seed), 15)
    return {
        "tokens": draw_tokens(jax.random.fold_in(key_of[14], 71), 0),
        "lengths": ragged_sizes(key_of[1], SEQS, SEQS * 7, STEP, 2).astype(jnp.int32),
        "norm_gain": jnp.clip(1.0 + 0.18 * jax.random.normal(key_of[2], (2, D), jnp.float32), 0.1, 1.9),
        "query_weight": bell_draw(key_of[3], (2, D, W), D ** -0.5, 0.09375, ((1, 4), (2, 8))),
        "key_weight": bell_draw(key_of[4], (2, D, W), D ** -0.5, 0.09375, ((1, 4), (2, 8))),
        "value_weight": bell_draw(key_of[5], (2, D, W), D ** -0.5, 0.09375, ((1, 4), (2, 8))),
        "outgate_weight": bell_draw(key_of[6], (2, D, W), D ** -0.5, 0.09375, ((1, 4), (2, 8))),
        "input_gate_weight": bell_draw(key_of[7], (2, D, HEADS), D ** -0.5, 0.09375),
        "forget_gate_weight": bell_draw(key_of[8], (2, D, HEADS), D ** -0.5, 0.09375),
        "forget_bias": jnp.clip(-1.0 + 7.0 * jax.random.uniform(key_of[9], (2, HEADS), jnp.float32) ** shard_levels(key_of[9], (2, HEADS), ((1, 8),), -0.2, 0.2), -1.0, 6.0),
        "out_weight": bell_draw(key_of[10], (2, W, D), W ** -0.5, 0.09375, ((1, 8), (2, 4))),
        "cell_state": bell_draw(key_of[11], (2, SEQS, HEADS, HEAD_DIM, HEAD_DIM), 0.25, 1.5, ((1, 4), (2, 8)), jnp.float32),
        "norm_state": bell_draw(key_of[12], (2, SEQS, HEADS, HEAD_DIM), 0.25, 1.5, ((1, 4), (2, 8)), jnp.float32),
        "max_state": bell_draw(key_of[13], (2, SEQS, HEADS), 1.0, 6.0, ((1, 4), (2, 8)), jnp.float32),
    }


EPSILON = 1e-06
NEG_FILL = -1e+30

def cell_update(cell, normer, stabil, query, key_vec, value, in_gate, log_forget, live):
    high = lax.Precision.HIGHEST
    in_gate = jnp.where(live, in_gate, NEG_FILL)
    log_forget = jnp.where(live, log_forget, 0.0)
    cumul = jnp.cumsum(log_forget, axis=-1)
    span = query.shape[2]
    causal = jnp.tril(jnp.ones((span, span), dtype=bool))
    log_weight = jnp.where(causal, cumul[..., :, None] - cumul[..., None, :] + in_gate[..., None, :], NEG_FILL)
    carried = cumul + stabil[..., None]
    running = jnp.maximum(lax.optimization_barrier(jnp.max(log_weight, axis=-1)), carried)
    carry_scale = jnp.exp(carried - running)
    scores = jnp.einsum('bhtd,bhud->bhtu', query, key_vec, precision=high) * jnp.exp(log_weight - running[..., None])
    numer = jnp.einsum('bhtu,bhue->bhte', scores, value, precision=high)
    numer = numer + carry_scale[..., None] * jnp.einsum('bhtd,bhde->bhte', query, cell, precision=high)
    denom = lax.optimization_barrier(jnp.sum(scores, axis=-1)) + carry_scale * jnp.einsum('bhtd,bhd->bht', query, normer, precision=high)
    readout = numer / jnp.maximum(jnp.abs(denom), 1.0)[..., None]
    readout = jnp.where(live[..., None], readout, 0.0)
    stabil_next = running[..., -1]
    source_weight = jnp.exp(cumul[..., -1:] - cumul + in_gate - stabil_next[..., None])
    decay = jnp.exp(cumul[..., -1] + stabil - stabil_next)
    cell_next = decay[..., None, None] * cell + jnp.einsum('bhu,bhud,bhue->bhde', source_weight, key_vec, value, precision=high)
    normer_next = decay[..., None] * normer + jnp.einsum('bhu,bhud->bhd', source_weight, key_vec, precision=high)
    return (cell_next, normer_next, stabil_next, readout)

def summed_blocks(scaled, weight, pieces):
    rows_each = scaled.shape[1] // pieces
    total = jnp.zeros((scaled.shape[0], weight.shape[1]), jnp.float32)
    for piece_index in range(pieces):
        lower = piece_index * rows_each
        part = jnp.dot(scaled[:, lower:lower + rows_each], weight[lower:lower + rows_each], preferred_element_type=jnp.float32)
        total = total + lax.optimization_barrier(part.astype(jnp.bfloat16)).astype(jnp.float32)
    return total

def to_heads(flat, seqs, span, heads):
    return jnp.transpose(flat.reshape(seqs, span, heads, -1), (0, 2, 1, 3)).astype(jnp.float32)

def reference(tokens, lengths, norm_gain, query_weight, key_weight, value_weight, outgate_weight, input_gate_weight, forget_gate_weight, forget_bias, out_weight, cell_state, norm_state, max_state):
    seqs, span, width = tokens.shape
    heads = cell_state.shape[2]
    head_size = cell_state.shape[3]
    live = (jnp.arange(span, dtype=jnp.int32)[None, :] < lengths[:, None])[:, None, :]
    current = tokens
    cells, normers, stabils = ([], [], [])
    for layer_index in range(2):
        flat = current.reshape(seqs * span, width)
        widened = flat.astype(jnp.float32)
        scale = lax.rsqrt(lax.optimization_barrier(jnp.mean(widened * widened, axis=-1, keepdims=True)) + EPSILON)
        scaled = (widened * norm_gain[layer_index]).astype(jnp.bfloat16)

        def project(weight):
            return (scale * summed_blocks(scaled, weight, N_DP)).astype(jnp.bfloat16)
        query = to_heads(project(query_weight[layer_index]), seqs, span, heads)
        key_vec = to_heads(project(key_weight[layer_index]), seqs, span, heads) * head_size ** (-0.5)
        value = to_heads(project(value_weight[layer_index]), seqs, span, heads)
        outgate = project(outgate_weight[layer_index]).astype(jnp.float32)
        gate_weights = jnp.concatenate([input_gate_weight[layer_index], forget_gate_weight[layer_index]], axis=1)
        gate_both = scale * summed_blocks(scaled, gate_weights, N_DP)
        in_gate = jnp.transpose(gate_both[:, :heads].reshape(seqs, span, heads), (0, 2, 1))
        log_forget = jax.nn.log_sigmoid(jnp.transpose(gate_both[:, heads:].reshape(seqs, span, heads) + forget_bias[layer_index], (0, 2, 1)))
        cell_next, normer_next, stabil_next, readout = cell_update(cell_state[layer_index], norm_state[layer_index], max_state[layer_index], query, key_vec, value, in_gate, log_forget, live)
        cells.append(cell_next)
        normers.append(normer_next)
        stabils.append(stabil_next)
        readout = jnp.transpose(readout, (0, 2, 1, 3)).reshape(seqs * span, heads * head_size)
        gated = (readout * jax.nn.sigmoid(outgate)).astype(jnp.bfloat16)
        mixed = jnp.dot(gated, out_weight[layer_index], preferred_element_type=jnp.float32)
        current = (widened + mixed).astype(jnp.bfloat16).reshape(seqs, span, width)
    return (current, jnp.stack(cells), jnp.stack(normers), jnp.stack(stabils))
```

```python
import functools
import jax
import jax.numpy as jnp
from jax import lax
from jax.experimental import pallas as pl
from jax.experimental.pallas import tpu as pltpu
from jax.sharding import PartitionSpec as P

EPSILON = 1e-06
NEG_FILL = -1e30
LANES = 128
HIGH = lax.Precision.HIGHEST
BF16 = jnp.bfloat16
F32 = jnp.float32
MESH = pl.DeviceIdType.MESH


def pack_squares(block):
    lane = lax.broadcasted_iota(jnp.int32, block.shape, 1)
    square = jnp.sum(jnp.where(lane >= LANES - 3, block, 0.0), axis=1, keepdims=True)
    first = square.astype(BF16).astype(F32)
    rest = square - first
    second = rest.astype(BF16).astype(F32)
    third = rest - second
    block = jnp.where(lane == LANES - 3, first, block)
    block = jnp.where(lane == LANES - 2, second, block)
    return jnp.where(lane == LANES - 1, third, block).astype(BF16)


def kernel(
    sizes,
    lengths,
    tokens,
    gain,
    weight_q,
    weight_k,
    weight_v,
    weight_o,
    weight_in,
    weight_forget,
    bias,
    weight_out,
    cell_in,
    norm_in,
    max_in,
    tokens_out,
    cells,
    norm_out,
    max_out,
    current,
    wts,
    wgate,
    wout,
    pad,
    gathered,
    scaled,
    own_main,
    own_gate,
    send1,
    send1g,
    recv1,
    recv1g,
    send2,
    send2g,
    recv2,
    recv2g,
    heads_buf,
    gated,
    mixed,
    mixed_s,
    mixed_y,
    mixed_in,
    load_sem,
    gat_s,
    gat_r,
    gfw_s,
    gfw_r,
    one_s,
    one_r,
    two_s,
    two_r,
    gg_s,
    gg_r,
    fw_s,
    fw_r,
    mix_s,
    mix_r,
    my_s,
    my_r,
):
    n_tp, n_dp, span, heads, size = sizes
    chips = n_dp // 2
    my_tp, my_dp = lax.axis_index("tp"), lax.axis_index("dp")
    my_x, my_core = my_dp // 2, lax.rem(my_dp, 2)
    peer_core = 1 - my_core
    peer = my_x * 2 + peer_core
    own_rows, feat = current.shape
    seqs = cell_in.shape[1]
    rows = seqs * span
    cols = heads * size
    main = (weight_q, weight_k, weight_v, weight_o)

    def loads(l):
        out = [
            pltpu.make_async_copy(w.at[l], wts.at[l, i], load_sem.at[l, i])
            for i, w in enumerate(main)
        ]
        start = pl.multiple_of(my_dp * feat, feat)
        for i, w in enumerate((weight_in, weight_forget)):
            out.append(
                pltpu.make_async_copy(
                    w.at[l, :, pl.ds(start, feat)], wgate.at[l, i], load_sem.at[l, 4 + i]
                )
            )
        out.append(pltpu.make_async_copy(cell_in.at[l], cells.at[l], load_sem.at[l, 6]))
        out.append(pltpu.make_async_copy(weight_out.at[l], wout.at[l], load_sem.at[l, 7]))
        return out

    for l in range(2):
        for copy in loads(l):
            copy.start()
    current[...] = tokens[...]

    y_size = chips if n_tp % chips == 0 else 1
    z_size = n_tp // y_size
    my_z, my_y = my_tp // y_size, lax.rem(my_tp, y_size)
    others_y = [lax.rem(my_y + j, y_size) for j in range(1, y_size)]
    others_z = [lax.rem(my_z + j, z_size) for j in range(1, z_size)]
    others_tp = [my_z * y_size + y for y in others_y] + [z * y_size + my_y for z in others_z]
    others_x = [lax.rem(my_x + j, chips) for j in range(1, chips)]
    barrier = pltpu.get_barrier_semaphore()
    for t in others_tp:
        pl.semaphore_signal(barrier, inc=1, device_id={"tp": t}, device_id_type=MESH)
    for x in others_x:
        pl.semaphore_signal(
            barrier, inc=1, device_id={"dp": x * 2 + my_core}, device_id_type=MESH
        )
    pl.semaphore_signal(barrier, inc=1, device_id={"dp": peer}, device_id_type=MESH)
    pl.semaphore_wait(barrier, len(others_tp) + chips)

    row_id = lax.broadcasted_iota(jnp.int32, (rows, rows), 0)
    col_id = lax.broadcasted_iota(jnp.int32, (rows, rows), 1)
    allowed = (row_id // span == col_id // span) & (col_id <= row_id)
    lane = lax.broadcasted_iota(jnp.int32, (rows, LANES), 1)
    row_l = lax.broadcasted_iota(jnp.int32, (rows, LANES), 0)
    reach = jnp.zeros((rows, LANES), jnp.int32)
    for b in range(seqs):
        reach = jnp.where(row_l // span == b, lengths[b], reach)
    live = lax.rem(row_l, span) < reach

    def remote(src, dst, s, r, where):
        return pltpu.make_async_remote_copy(
            src_ref=src, dst_ref=dst, send_sem=s, recv_sem=r, device_id=where, device_id_type=MESH
        )

    def tp_rows(t):
        return pl.ds(pl.multiple_of(t * own_rows, own_rows), own_rows)

    def layer(l, carry):
        def gather_z(source, target):
            return remote(
                current,
                gathered.at[l, tp_rows(source * y_size + my_y)],
                gat_s.at[l, target],
                gat_r.at[l, source],
                {"tp": target * y_size + my_y},
            )

        def gather_y(z, source, target):
            part = gathered.at[l, tp_rows(z * y_size + source)]
            return remote(
                part,
                part,
                gfw_s.at[l, z, target],
                gfw_r.at[l, z, source],
                {"tp": my_z * y_size + target},
            )

        def gather_own(source, target):
            return remote(
                current,
                gathered.at[l, tp_rows(my_z * y_size + source)],
                gfw_s.at[l, my_z, target],
                gfw_r.at[l, my_z, source],
                {"tp": my_z * y_size + target},
            )

        for z in others_z:
            gather_z(my_z, z).start()
        for y in others_y:
            gather_own(my_y, y).start()
        gathered[l, tp_rows(my_tp)] = current[...]
        incoming = loads(l)
        for copy in incoming[4:6]:
            copy.wait()
        total_heads = wgate.shape[2]
        pick_r = lax.broadcasted_iota(jnp.int32, (LANES, total_heads), 1)
        pick_c = lax.broadcasted_iota(jnp.int32, (LANES, total_heads), 0)
        head_start = my_tp * heads
        pick_in = ((pick_r == head_start + pick_c) & (pick_c < heads)).astype(F32).astype(BF16)
        pick_fg = (
            ((pick_r == head_start + pick_c - heads) & (pick_c >= heads) & (pick_c < 2 * heads))
            .astype(F32)
            .astype(BF16)
        )
        gate_w = (
            jnp.dot(pick_in, wgate[l, 0], preferred_element_type=F32)
            + jnp.dot(pick_fg, wgate[l, 1], preferred_element_type=F32)
        ).astype(BF16)
        for copy in incoming[:4]:
            copy.wait()
        for z in reversed(others_z):
            gather_z(z, z).wait_recv()
            for y in others_y:
                gather_y(z, my_y, y).start()
        for z in [my_z] + others_z:
            for y in others_y:
                gather_y(z, y, y).wait_recv()

        gain_row = gain[pl.ds(l, 1), :]
        for d in range(n_dp):
            block = gathered[l, d * rows : (d + 1) * rows].astype(F32)
            core, x = d % 2, d // 2
            scaled[core, x * rows : (x + 1) * rows] = (block * gain_row).astype(BF16)
            own_gate[core, x * rows : (x + 1) * rows] = jnp.broadcast_to(
                jnp.sum(block * block, axis=1, keepdims=True), (rows, LANES)
            )
        lane_all = lax.broadcasted_iota(jnp.int32, (chips * rows, LANES), 1)
        for core in range(2):
            part = lax.dot_general(
                scaled[core], gate_w, (((1,), (1,)), ((), ())), preferred_element_type=F32
            )
            part = jnp.where(lane_all == LANES - 3, own_gate[core], part)
            own_gate[core] = part
        send1g[...] = pack_squares(own_gate[peer_core])

        def one_gate():
            return remote(
                send1g, recv1g.at[l], one_s.at[l, 4], one_r.at[l, 4], {"dp": peer}
            )

        def one_main(c):
            return remote(
                send1.at[c], recv1.at[l, c], one_s.at[l, c], one_r.at[l, c], {"dp": peer}
            )

        def x_rows(x):
            return pl.ds(pl.multiple_of(x * rows, rows), rows)

        def two_gate(source, target):
            return remote(
                send2g.at[x_rows(target)],
                recv2g.at[l, source],
                two_s.at[l, 4, target],
                two_r.at[l, 4, source],
                {"dp": target * 2 + my_core},
            )

        def two_main(c, source, target):
            return remote(
                send2.at[c, x_rows(target)],
                recv2.at[l, c, source],
                two_s.at[l, c, target],
                two_r.at[l, c, source],
                {"dp": target * 2 + my_core},
            )

        one_gate().start()
        one_gate().wait_recv()
        both = own_gate[my_core] + recv1g[l].astype(F32)
        own_gate[my_core] = both
        send2g[...] = pack_squares(both)
        for x in others_x:
            two_gate(my_x, x).start()

        def project(c, carry):
            send1[c] = jnp.dot(
                scaled[peer_core], wts[l, c], preferred_element_type=F32
            ).astype(BF16)
            one_main(c).start()
            own = jnp.dot(scaled[my_core], wts[l, c], preferred_element_type=F32)
            one_main(c).wait_recv()
            own = own + recv1[l, c].astype(F32)
            own_main[c] = own
            send2[c] = own.astype(BF16)
            for x in others_x:
                two_main(c, my_x, x).start()
            return carry

        lax.fori_loop(0, 4, project, 0)
        incoming[6].wait()
        for x in others_x:
            two_gate(x, x).wait_recv()

        sums = own_gate[my_core, x_rows(my_x)]
        for x in others_x:
            sums = sums + recv2g[l, x].astype(F32)
        square = jnp.sum(jnp.where(lane >= LANES - 3, sums, 0.0), axis=1, keepdims=True)
        scale = lax.rsqrt(square / (feat * n_dp) + EPSILON)
        gates = scale * sums
        pad[...] = jnp.zeros_like(pad)
        pad[0:seqs, 0:heads] = jnp.transpose(max_in[l])
        pad[seqs : seqs + 1, 0:heads] = bias[pl.ds(l, 1), :]
        stabil = pad[0:seqs, :]
        forget = pltpu.roll(gates, LANES - heads, 1) + pad[seqs : seqs + 1, :]
        log_forget = jnp.minimum(forget, 0.0) - jnp.log1p(jnp.exp(-jnp.abs(forget)))
        in_gate = jnp.where(live, gates, NEG_FILL)
        log_forget = jnp.where(live, log_forget, 0.0)
        cumul = jnp.dot(
            allowed.astype(F32), log_forget, preferred_element_type=F32, precision=HIGH
        )

        def spread(value):
            wide = jnp.broadcast_to(value[:, None, :], (seqs, span, value.shape[-1]))
            return wide.reshape(rows, value.shape[-1])

        def last(value):
            return value.reshape(seqs, span, value.shape[-1])[:, span - 1, :]

        carried = cumul + spread(stabil)
        source = jnp.transpose(in_gate - cumul)

        for c in range(4):
            for x in others_x:
                two_main(c, x, x).wait_recv()
            full = own_main[c, x_rows(my_x)]
            for x in others_x:
                full = full + recv2[l, c, x].astype(F32)
            heads_buf[c] = (scale * full).astype(BF16)

        key_scale = size ** (-0.5)
        normer = norm_in[l]
        running = jnp.zeros((rows, LANES), F32)
        for h in range(heads):
            span_h = slice(h * size, (h + 1) * size)
            q, k, v = (heads_buf[c, :, span_h] for c in range(3))
            weight = jnp.where(allowed, cumul[:, h : h + 1] + source[h : h + 1, :], NEG_FILL)
            top = jnp.maximum(jnp.max(weight, axis=1, keepdims=True), carried[:, h : h + 1])
            running = jnp.where(lane == h, top, running)
            decay = jnp.exp(carried[:, h : h + 1] - top)
            scores = lax.dot_general(
                q, k, (((1,), (1,)), ((), ())), preferred_element_type=F32
            )
            scores = scores * key_scale * jnp.exp(weight - top)
            numer = jnp.dot(scores.astype(BF16), v, preferred_element_type=F32)
            from_cell = jnp.concatenate(
                [
                    jnp.dot(
                        q[b * span : (b + 1) * span],
                        cells[l, b, h].astype(BF16),
                        preferred_element_type=F32,
                    )
                    for b in range(seqs)
                ],
                axis=0,
            )
            numer = numer + decay * from_cell
            from_norm = jnp.sum(
                q.astype(F32) * spread(normer[:, h, :]), axis=1, keepdims=True
            )
            denom = jnp.sum(scores, axis=1, keepdims=True) + decay * from_norm
            readout = numer / jnp.maximum(jnp.abs(denom), 1.0)
            readout = jnp.where(live, readout, 0.0)
            outgate = heads_buf[3, :, span_h].astype(F32)
            gated[l, my_dp, :, span_h] = (readout / (1.0 + jnp.exp(-outgate))).astype(BF16)

        def across(source, target):
            return remote(
                gated.at[l, source],
                gated.at[l, source],
                gg_s.at[l, target // 2],
                gg_r.at[l, source // 2],
                {"dp": target},
            )

        def inside(block, x):
            return remote(
                gated.at[l, block], gated.at[l, block], fw_s.at[l, x], fw_r.at[l, x], {"dp": peer}
            )

        for x in others_x:
            across(my_dp, x * 2 + my_core).start()
        inside(my_dp, my_x).start()

        top_last, cumul_last = last(running), last(cumul)
        weights = jnp.exp(spread(cumul_last - top_last) - cumul + in_gate)
        fade = jnp.exp(cumul_last + stabil - top_last)
        max_out[l] = jnp.transpose(top_last)[0:heads, :]
        seq_col = lax.broadcasted_iota(jnp.int32, (size, rows), 1) // span
        pick = (
            lax.broadcasted_iota(jnp.int32, (seqs, rows), 1) // span
            == lax.broadcasted_iota(jnp.int32, (seqs, rows), 0)
        ).astype(F32)
        for h in range(heads):
            span_h = slice(h * size, (h + 1) * size)
            v = heads_buf[2, :, span_h]
            k = heads_buf[1, :, span_h].astype(F32) * key_scale * weights[:, h : h + 1]
            flipped = jnp.transpose(k)
            stacked = jnp.concatenate(
                [jnp.where(seq_col == b, flipped, 0.0).astype(BF16) for b in range(seqs)], axis=0
            )
            added = jnp.dot(stacked, v, preferred_element_type=F32)
            for b in range(seqs):
                cells[l, b, h] = (
                    fade[b : b + 1, h : h + 1] * cells[l, b, h]
                    + added[b * size : (b + 1) * size]
                )
            norm_out[l, :, h, :] = fade[:, h : h + 1] * normer[:, h, :] + jnp.dot(
                pick, k, preferred_element_type=F32, precision=HIGH
            )

        for x in others_x:
            across(x * 2 + my_core, x * 2 + my_core).wait_recv()
            inside(x * 2 + my_core, x).start()
        incoming[7].wait()
        for x in [my_x] + others_x:
            inside(x * 2 + peer_core, x).wait_recv()

        def mix(d, carry):
            part = jnp.dot(gated[l, d], wout[l], preferred_element_type=F32)
            mixed[pl.ds(pl.multiple_of(d * rows, rows), rows), :] = part.astype(BF16)
            return carry

        lax.fori_loop(0, n_dp, mix, 0)

        def scatter_y(z, source, target):
            return remote(
                mixed.at[tp_rows(z * y_size + target)],
                mixed_y.at[l, z, source],
                my_s.at[l, z, target],
                my_r.at[l, z, source],
                {"tp": my_z * y_size + target},
            )

        def scatter_z(source, target):
            return remote(
                mixed_s.at[target],
                mixed_in.at[l, source],
                mix_s.at[l, target],
                mix_r.at[l, source],
                {"tp": target * y_size + my_y},
            )

        for z in others_z + [my_z]:
            for y in others_y:
                scatter_y(z, my_y, y).start()
        for z in others_z:
            gather_z(my_z, z).wait_send()
            for y in others_y:
                gather_y(z, my_y, y).wait_send()
        for y in others_y:
            gather_own(my_y, y).wait_send()
        one_gate().wait_send()
        for c in range(4):
            one_main(c).wait_send()
        for x in others_x:
            two_gate(my_x, x).wait_send()
            for c in range(4):
                two_main(c, my_x, x).wait_send()
            across(my_dp, x * 2 + my_core).wait_send()
        for x in [my_x] + others_x:
            inside(x * 2 + my_core, x).wait_send()
        for z in others_z + [my_z]:
            total = mixed[tp_rows(z * y_size + my_y), :].astype(F32)
            for y in others_y:
                scatter_y(z, y, y).wait_recv()
                total = total + mixed_y[l, z, y].astype(F32)
            if z is not my_z:
                mixed_s[z] = total.astype(BF16)
                scatter_z(my_z, z).start()
        for z in reversed(others_z):
            scatter_z(z, z).wait_recv()
            total = total + mixed_in[l, z].astype(F32)
        current[...] = (current[...].astype(F32) + total).astype(BF16)
        for z in others_z:
            scatter_z(my_z, z).wait_send()
        for z in others_z + [my_z]:
            for y in others_y:
                scatter_y(z, my_y, y).wait_send()
        return carry

    lax.fori_loop(0, 2, layer, 0)
    tokens_out[...] = current[...]


def store(*refs):
    sem = refs[-1]
    copies = [pltpu.make_async_copy(refs[i], refs[4 + i], sem.at[i]) for i in range(4)]
    for copy in copies:
        copy.start()
    for copy in copies:
        copy.wait()


def per_device(
    tokens,
    lengths,
    norm_gain,
    query_weight,
    key_weight,
    value_weight,
    outgate_weight,
    input_gate_weight,
    forget_gate_weight,
    forget_bias,
    out_weight,
    cell_state,
    norm_state,
    max_state,
):
    n_tp, n_dp = lax.axis_size("tp"), lax.axis_size("dp")
    seq_here, span, feat = tokens.shape
    seqs, heads, size = cell_state.shape[1:4]
    own_rows, rows, cols, chips = seq_here * span, seqs * span, heads * size, n_dp // 2
    everyone = n_tp * own_rows
    n_y = chips if n_tp % chips == 0 else 1
    n_z = n_tp // n_y
    vmem = pl.BlockSpec(memory_space=pltpu.VMEM)
    smem = pl.BlockSpec(memory_space=pltpu.SMEM)
    hbm = pl.BlockSpec(memory_space=pl.ANY)
    V, sem = pltpu.VMEM, pltpu.SemaphoreType.DMA
    result = pl.pallas_call(
        functools.partial(kernel, (n_tp, n_dp, span, heads, size)),
        out_shape=(
            V((own_rows, feat), BF16),
            V(cell_state.shape, F32),
            V(norm_state.shape, F32),
            V((2, heads, seqs), F32),
        ),
        in_specs=[smem, vmem, vmem, hbm, hbm, hbm, hbm, hbm, hbm, vmem, hbm, hbm, vmem, vmem],
        out_specs=(vmem, vmem, vmem, vmem),
        scratch_shapes=[
            V((own_rows, feat), BF16),
            V((2, 4, feat, cols), BF16),
            V((2, 2, input_gate_weight.shape[2], feat), BF16),
            V((2, cols, feat), BF16),
            V((seqs + 8, LANES), F32),
            V((2, everyone, feat), BF16),
            V((2, chips * rows, feat), BF16),
            V((4, chips * rows, cols), F32),
            V((2, chips * rows, LANES), F32),
            V((4, chips * rows, cols), BF16),
            V((chips * rows, LANES), BF16),
            V((2, 4, chips * rows, cols), BF16),
            V((2, chips * rows, LANES), BF16),
            V((4, chips * rows, cols), BF16),
            V((chips * rows, LANES), BF16),
            V((2, 4, chips, rows, cols), BF16),
            V((2, chips, rows, LANES), BF16),
            V((4, rows, cols), BF16),
            V((2, n_dp, rows, cols), BF16),
            V((everyone, feat), BF16),
            V((n_z, own_rows, feat), BF16),
            V((2, n_z, n_y, own_rows, feat), BF16),
            V((2, n_z, own_rows, feat), BF16),
            sem((2, 8)),
            sem((2, n_z)),
            sem((2, n_z)),
            sem((2, n_z, n_y)),
            sem((2, n_z, n_y)),
            sem((2, 5)),
            sem((2, 5)),
            sem((2, 5, chips)),
            sem((2, 5, chips)),
            sem((2, chips)),
            sem((2, chips)),
            sem((2, chips)),
            sem((2, chips)),
            sem((2, n_z)),
            sem((2, n_z)),
            sem((2, n_z, n_y)),
            sem((2, n_z, n_y)),
        ],
        compiler_params=pltpu.CompilerParams(
            collective_id=0, has_side_effects=True, vmem_limit_bytes=48 * 1024 * 1024
        ),
    )(
        lengths,
        tokens.reshape(own_rows, feat),
        norm_gain,
        query_weight,
        key_weight,
        value_weight,
        outgate_weight,
        jnp.swapaxes(input_gate_weight, 1, 2),
        jnp.swapaxes(forget_gate_weight, 1, 2),
        forget_bias,
        out_weight,
        cell_state,
        norm_state,
        jnp.swapaxes(max_state, 1, 2),
    )
    result = pl.pallas_call(
        store,
        out_shape=tuple(jax.ShapeDtypeStruct(part.shape, part.dtype) for part in result),
        in_specs=[vmem] * 4,
        out_specs=(hbm,) * 4,
        scratch_shapes=[sem((4,))],
        compiler_params=pltpu.CompilerParams(vmem_limit_bytes=16 * 1024 * 1024),
    )(*result)
    return (result[0].reshape(tokens.shape), *result[1:3], jnp.swapaxes(result[3], 1, 2))


def solution(mesh):
    return jax.shard_map(
        per_device,
        mesh=mesh,
        in_specs=(
            P("tp", None, "dp"),
            P("dp"),
            P(None, "dp"),
            P(None, "dp", "tp"),
            P(None, "dp", "tp"),
            P(None, "dp", "tp"),
            P(None, "dp", "tp"),
            P(),
            P(),
            P(None, "tp"),
            P(None, "tp", "dp"),
            P(None, "dp", "tp", None, None),
            P(None, "dp", "tp", None),
            P(None, "dp", "tp"),
        ),
        out_specs=(
            P("tp", None, "dp"),
            P(None, "dp", "tp", None, None),
            P(None, "dp", "tp", None),
            P(None, "dp", "tp"),
        ),
        check_vma=False,
    )
```

```python
import functools
import jax
import jax.numpy as jnp
from jax import lax
from jax.experimental import pallas as pl
from jax.experimental.pallas import tpu as pltpu
from jax.sharding import PartitionSpec as P

EPSILON = 1e-06
NEG_FILL = -1e30
LANES = 128
HIGH = lax.Precision.HIGHEST
BF16 = jnp.bfloat16
F32 = jnp.float32
MESH = pl.DeviceIdType.MESH
BATCHES = 2
LAYERS = 2
ISSUE = {
    "forward": 3.0,
    "project": 12.0,
    "exchange": 12.1,
    "attend": 21.0,
    "relay": 25.0,
    "mix": 28.0,
    "fold": 31.0,
    "finish": 40.0,
}
LAG = 5.6
PERIOD = 40.5


def pack_squares(block):
    lane = lax.broadcasted_iota(jnp.int32, block.shape, 1)
    square = jnp.sum(jnp.where(lane >= LANES - 3, block, 0.0), axis=1, keepdims=True)
    first = square.astype(BF16).astype(F32)
    rest = square - first
    second = rest.astype(BF16).astype(F32)
    third = rest - second
    block = jnp.where(lane == LANES - 3, first, block)
    block = jnp.where(lane == LANES - 2, second, block)
    return jnp.where(lane == LANES - 1, third, block).astype(BF16)


def flip_bits(value, mask):
    result = value
    bit = 1
    while bit <= mask:
        if mask & bit:
            result = result + bit * (1 - 2 * lax.rem(value // bit, 2))
        bit = bit * 2
    return result


def kernel(sizes, *refs):
    n_tp, n_dp, span, heads, size, n_y, names = sizes
    r = dict(zip(names, refs))
    lengths, norm, stabils, gain = r["lengths"], r["norm"], r["stabils"], r["gain"]
    cells, norm_out, max_out, tokens_out = r["cells"], r["norm_out"], r["max_out"], r["tokens_out"]
    current, wts, wgate, wout = r["current"], r["wts"], r["wgate"], r["wout"]
    gathered, scaled, gate_w, both = r["gathered"], r["scaled"], r["gate_w"], r["both"]
    own_gate, own_main, heads_buf = r["own_gate"], r["own_main"], r["heads_buf"]
    gated, mixed, top_buf, pad = r["gated"], r["mixed"], r["top_buf"], r["pad"]
    load_sem = r["load_sem"]
    chips = n_dp // 2
    n_z = n_tp // n_y
    my_tp, my_dp = lax.axis_index("tp"), lax.axis_index("dp")
    my_x, my_core = my_dp // 2, lax.rem(my_dp, 2)
    peer_core = 1 - my_core
    peer = my_x * 2 + peer_core
    my_z, my_y = my_tp // n_y, lax.rem(my_tp, n_y)
    own_rows, feat = current.shape[2:]
    seqs = cells.shape[1]
    own_part = own_rows // span
    own_seqs = own_part * BATCHES
    ratio = seqs // own_seqs
    seqs_b = seqs // BATCHES
    rows = seqs_b * span
    total_rows = n_dp * rows
    key_scale = size ** (-0.5)

    def load(index, source, target):
        return pltpu.make_async_copy(source, target, load_sem.at[index])

    start = pl.multiple_of(my_dp * feat, feat)
    small = [
        load(0, r["tokens"], current.at[0]),
        load(1, r["lengths_in"], lengths),
        load(2, r["gain_in"], gain),
        load(3, r["norm_in"], norm),
        load(4, r["max_in"], stabils),
        load(5, r["bias_in"], r["bias"]),
    ]
    big = []
    for l in range(LAYERS):
        part = []
        for i, name in enumerate(("weight_in", "weight_forget")):
            part.append(load(6 + 8 * l + i, r[name].at[l, :, pl.ds(start, feat)], wgate.at[l, i]))
        for i, name in enumerate(("weight_q", "weight_k", "weight_v", "weight_o")):
            part.append(load(8 + 8 * l + i, r[name].at[l], wts.at[l, i]))
        part.append(load(12 + 8 * l, r["cell_in"].at[l], cells.at[l]))
        part.append(load(13 + 8 * l, r["weight_out"].at[l], wout.at[l]))
        big.append(part)
    for copy in small + big[0] + big[1]:
        copy.start()

    others_y = [lax.rem(my_y + j, n_y) for j in range(1, n_y)]
    power = n_z & (n_z - 1) == 0
    others_z = [flip_bits(my_z, j) if power else lax.rem(my_z + j, n_z) for j in range(1, n_z)]
    sources_z = others_z if power else [lax.rem(my_z + n_z - j, n_z) for j in range(1, n_z)]
    others_tp = [my_z * n_y + y for y in others_y] + [z * n_y + my_y for z in others_z]
    others_x = [lax.rem(my_x + j, chips) for j in range(1, chips)]
    barrier = pltpu.get_barrier_semaphore()
    for t in others_tp:
        pl.semaphore_signal(barrier, inc=1, device_id={"tp": t}, device_id_type=MESH)
    for x in others_x:
        pl.semaphore_signal(
            barrier, inc=1, device_id={"dp": x * 2 + my_core}, device_id_type=MESH
        )
    pl.semaphore_signal(barrier, inc=1, device_id={"dp": peer}, device_id_type=MESH)
    pl.semaphore_wait(barrier, len(others_tp) + chips)

    def remote(src, dst, s, rcv, where):
        return pltpu.make_async_remote_copy(
            src_ref=src, dst_ref=dst, send_sem=s, recv_sem=rcv, device_id=where, device_id_type=MESH
        )

    def tp_rows(t):
        return pl.ds(pl.multiple_of(t * own_rows, own_rows), own_rows)

    def x_rows(x):
        return pl.ds(pl.multiple_of(x * rows, rows), rows)

    def gather_z(l, b, source, target):
        return remote(
            current.at[l, b],
            gathered.at[l, b, tp_rows(source * n_y + my_y)],
            r["gat_s"].at[l, b, target],
            r["gat_r"].at[l, b, source],
            {"tp": target * n_y + my_y},
        )

    def gather_y(l, b, z, source, target, own=False):
        part = gathered.at[l, b, tp_rows(z * n_y + source)]
        return remote(
            current.at[l, b] if own else part,
            part,
            r["gfw_s"].at[l, b, z, target],
            r["gfw_r"].at[l, b, z, source],
            {"tp": my_z * n_y + target},
        )

    def one_gate(l, b):
        return remote(
            r["send1g"].at[l, b],
            r["recv1g"].at[l, b],
            r["one_s"].at[l, b, 4],
            r["one_r"].at[l, b, 4],
            {"dp": peer},
        )

    def one_main(l, b, c):
        return remote(
            r["send1"].at[l, b, c],
            r["recv1"].at[l, b, c],
            r["one_s"].at[l, b, c],
            r["one_r"].at[l, b, c],
            {"dp": peer},
        )

    def two_gate(l, b, source, target):
        return remote(
            r["send2g"].at[l, b, x_rows(target)],
            r["recv2g"].at[l, b, source],
            r["two_s"].at[l, b, 4, target],
            r["two_r"].at[l, b, 4, source],
            {"dp": target * 2 + my_core},
        )

    def two_main(l, b, c, source, target):
        return remote(
            r["send2"].at[l, b, c, x_rows(target)],
            r["recv2"].at[l, b, c, source],
            r["two_s"].at[l, b, c, target],
            r["two_r"].at[l, b, c, source],
            {"dp": target * 2 + my_core},
        )

    def across(l, b, source, target):
        return remote(
            gated.at[l, b, source],
            gated.at[l, b, source],
            r["gg_s"].at[l, b, target // 2],
            r["gg_r"].at[l, b, source // 2],
            {"dp": target},
        )

    def inside(l, b, block, x):
        return remote(
            gated.at[l, b, block],
            gated.at[l, b, block],
            r["fw_s"].at[l, b, x],
            r["fw_r"].at[l, b, x],
            {"dp": peer},
        )

    def scatter_y(l, b, z, source, target):
        return remote(
            mixed.at[l, b, tp_rows(z * n_y + target)],
            r["mixed_y"].at[l, b, z, source],
            r["my_s"].at[l, b, z, target],
            r["my_r"].at[l, b, z, source],
            {"tp": my_z * n_y + target},
        )

    def scatter_z(l, b, source, target):
        return remote(
            r["mixed_s"].at[l, b, target],
            r["mixed_in"].at[l, b, source],
            r["mix_s"].at[l, b, target],
            r["mix_r"].at[l, b, source],
            {"tp": target * n_y + my_y},
        )

    def begin(l, b):
        for z in others_z:
            gather_z(l, b, my_z, z).start()
        for y in others_y:
            gather_y(l, b, my_z, my_y, y, own=True).start()
        gathered[l, b, tp_rows(my_tp)] = current[l, b]

    small[0].wait()
    for b in range(BATCHES):
        begin(0, b)
    for copy in small[1:]:
        copy.wait()

    row_id = lax.broadcasted_iota(jnp.int32, (rows, rows), 0)
    col_id = lax.broadcasted_iota(jnp.int32, (rows, rows), 1)
    allowed = (row_id // span == col_id // span) & (col_id <= row_id)
    lane = lax.broadcasted_iota(jnp.int32, (rows, LANES), 1)
    row_l = lax.broadcasted_iota(jnp.int32, (rows, LANES), 0)
    runs = [
        [slice(j * own_seqs + b * own_part, j * own_seqs + (b + 1) * own_part) for j in range(ratio)]
        for b in range(BATCHES)
    ]

    def live_of(b):
        reach = jnp.zeros((rows, LANES), jnp.int32)
        place = 0
        for run in runs[b]:
            for s in range(run.start, run.stop):
                reach = jnp.where(row_l // span == place, lengths[s], reach)
                place = place + 1
        return lax.rem(row_l, span) < reach

    pad[...] = jnp.zeros_like(pad)
    for l in range(LAYERS):
        pad[l, 0:seqs, 0:heads] = jnp.transpose(stabils[l])
        pad[l, seqs : seqs + 1, 0:heads] = r["bias"][l : l + 1, :]

    def spread(value):
        wide = jnp.broadcast_to(value[:, None, :], (seqs_b, span, value.shape[-1]))
        return wide.reshape(rows, value.shape[-1])

    def last(value):
        return value.reshape(seqs_b, span, value.shape[-1])[:, span - 1, :]

    def gate_columns(l):
        for copy in big[l][:2]:
            copy.wait()
        total_heads = wgate.shape[2]
        pick_r = lax.broadcasted_iota(jnp.int32, (LANES, total_heads), 1)
        pick_c = lax.broadcasted_iota(jnp.int32, (LANES, total_heads), 0)
        head_start = my_tp * heads
        pick_in = ((pick_r == head_start + pick_c) & (pick_c < heads)).astype(F32).astype(BF16)
        pick_fg = (
            ((pick_r == head_start + pick_c - heads) & (pick_c >= heads) & (pick_c < 2 * heads))
            .astype(F32)
            .astype(BF16)
        )
        gate_w[l] = (
            jnp.dot(pick_in, wgate[l, 0], preferred_element_type=F32)
            + jnp.dot(pick_fg, wgate[l, 1], preferred_element_type=F32)
        ).astype(BF16)

    for l in range(LAYERS):
        gate_columns(l)

    def forward(l, b, j):
        z = sources_z[j]
        gather_z(l, b, z, z).wait_recv()
        for y in others_y:
            gather_y(l, b, z, my_y, y).start()

    def project(l, b):
        for z in [my_z] + others_z:
            for y in others_y:
                gather_y(l, b, z, y, y).wait_recv()
        gain_row = gain[l : l + 1, :]
        for d in range(n_dp):
            block = gathered[l, b, d * rows : (d + 1) * rows].astype(F32)
            core, x = d % 2, d // 2
            scaled[core, x * rows : (x + 1) * rows] = (block * gain_row).astype(BF16)
            own_gate[b, core, x * rows : (x + 1) * rows] = jnp.broadcast_to(
                jnp.sum(block * block, axis=1, keepdims=True), (rows, LANES)
            )
        lane_all = lax.broadcasted_iota(jnp.int32, (chips * rows, LANES), 1)
        for core in range(2):
            part = lax.dot_general(
                scaled[core], gate_w[l], (((1,), (1,)), ((), ())), preferred_element_type=F32
            )
            own_gate[b, core] = jnp.where(lane_all == LANES - 3, own_gate[b, core], part)
        r["send1g"][l, b] = pack_squares(own_gate[b, peer_core])
        one_gate(l, b).start()
        if b == 0:
            for copy in big[l][2:6]:
                copy.wait()

        def one(c, carry):
            flat = scaled[...].reshape(2 * chips * rows, feat)
            both[...] = jnp.dot(flat, wts[l, c], preferred_element_type=F32).reshape(both.shape)
            r["send1"][l, b, c] = both[peer_core].astype(BF16)
            one_main(l, b, c).start()
            own_main[b, c] = both[my_core]
            return carry

        lax.fori_loop(0, 4, one, 0)

    def exchange(l, b):
        one_gate(l, b).wait_recv()
        summed = own_gate[b, my_core] + r["recv1g"][l, b].astype(F32)
        own_gate[b, my_core] = summed
        r["send2g"][l, b] = pack_squares(summed)
        for x in others_x:
            two_gate(l, b, my_x, x).start()

        def one(c, carry):
            one_main(l, b, c).wait_recv()
            own = own_main[b, c] + r["recv1"][l, b, c].astype(F32)
            own_main[b, c] = own
            r["send2"][l, b, c] = own.astype(BF16)
            for x in others_x:
                two_main(l, b, c, my_x, x).start()
            return carry

        lax.fori_loop(0, 4, one, 0)

    def attend(l, b):
        live = live_of(b)
        for x in others_x:
            two_gate(l, b, x, x).wait_recv()
        sums = own_gate[b, my_core, x_rows(my_x)]
        for x in others_x:
            sums = sums + r["recv2g"][l, b, x].astype(F32)
        square = jnp.sum(jnp.where(lane >= LANES - 3, sums, 0.0), axis=1, keepdims=True)
        scale = lax.rsqrt(square / (feat * n_dp) + EPSILON)
        gates = scale * sums
        stabil = jnp.concatenate([pad[l, run] for run in runs[b]], axis=0)
        forget = pltpu.roll(gates, LANES - heads, 1) + pad[l, seqs : seqs + 1, :]
        log_forget = jnp.minimum(forget, 0.0) - jnp.log1p(jnp.exp(-jnp.abs(forget)))
        in_gate = jnp.where(live, gates, NEG_FILL)
        log_forget = jnp.where(live, log_forget, 0.0)
        cumul = jnp.dot(
            allowed.astype(F32), log_forget, preferred_element_type=F32, precision=HIGH
        )
        carried = cumul + spread(stabil)
        source = jnp.transpose(in_gate - cumul)
        if b == 0:
            big[l][6].wait()
        for c in range(4):
            for x in others_x:
                two_main(l, b, c, x, x).wait_recv()
            full = own_main[b, c, x_rows(my_x)]
            for x in others_x:
                full = full + r["recv2"][l, b, c, x].astype(F32)
            heads_buf[b, c] = (scale * full).astype(BF16)

        ids = [s for run in runs[b] for s in range(run.start, run.stop)]
        running = jnp.zeros((rows, LANES), F32)
        for h in range(heads):
            span_h = slice(h * size, (h + 1) * size)
            normer = jnp.concatenate([norm[l, run, h, :] for run in runs[b]], axis=0)
            q, k, v = (heads_buf[b, c, :, span_h] for c in range(3))
            weight = jnp.where(allowed, cumul[:, h : h + 1] + source[h : h + 1, :], NEG_FILL)
            top = jnp.maximum(jnp.max(weight, axis=1, keepdims=True), carried[:, h : h + 1])
            running = jnp.where(lane == h, top, running)
            decay = jnp.exp(carried[:, h : h + 1] - top)
            scores = lax.dot_general(
                q, k, (((1,), (1,)), ((), ())), preferred_element_type=F32
            )
            scores = scores * key_scale * jnp.exp(weight - top)
            numer = jnp.dot(scores.astype(BF16), v, preferred_element_type=F32)
            from_cell = jnp.concatenate(
                [
                    jnp.dot(
                        q[i * span : (i + 1) * span],
                        cells[l, s, h].astype(BF16),
                        preferred_element_type=F32,
                    )
                    for i, s in enumerate(ids)
                ],
                axis=0,
            )
            numer = numer + decay * from_cell
            from_norm = jnp.sum(q.astype(F32) * spread(normer), axis=1, keepdims=True)
            denom = jnp.sum(scores, axis=1, keepdims=True) + decay * from_norm
            readout = numer / jnp.maximum(jnp.abs(denom), 1.0)
            readout = jnp.where(live, readout, 0.0)
            outgate = heads_buf[b, 3, :, span_h].astype(F32)
            gated[l, b, my_dp, :, span_h] = (readout / (1.0 + jnp.exp(-outgate))).astype(BF16)

        for x in others_x:
            across(l, b, my_dp, x * 2 + my_core).start()
        inside(l, b, my_dp, my_x).start()

        top_last, cumul_last = last(running), last(cumul)
        weights = jnp.exp(spread(cumul_last - top_last) - cumul + in_gate)
        fade = jnp.exp(cumul_last + stabil - top_last)
        for j, run in enumerate(runs[b]):
            top_buf[l, run] = top_last[j * own_part : (j + 1) * own_part]
        seq_col = lax.broadcasted_iota(jnp.int32, (size, rows), 1) // span
        pick = (
            lax.broadcasted_iota(jnp.int32, (seqs_b, rows), 1) // span
            == lax.broadcasted_iota(jnp.int32, (seqs_b, rows), 0)
        ).astype(F32)
        for h in range(heads):
            span_h = slice(h * size, (h + 1) * size)
            normer = jnp.concatenate([norm[l, run, h, :] for run in runs[b]], axis=0)
            v = heads_buf[b, 2, :, span_h]
            k = heads_buf[b, 1, :, span_h].astype(F32) * key_scale * weights[:, h : h + 1]
            flipped = jnp.transpose(k)
            stacked = jnp.concatenate(
                [jnp.where(seq_col == i, flipped, 0.0).astype(BF16) for i in range(seqs_b)], axis=0
            )
            added = jnp.dot(stacked, v, preferred_element_type=F32)
            for i, s in enumerate(ids):
                cells[l, s, h] = (
                    fade[i : i + 1, h : h + 1] * cells[l, s, h]
                    + added[i * size : (i + 1) * size]
                )
            moved = fade[:, h : h + 1] * normer + jnp.dot(
                pick, k, preferred_element_type=F32, precision=HIGH
            )
            for j, run in enumerate(runs[b]):
                norm_out[l, run, h, :] = moved[j * own_part : (j + 1) * own_part]

    def relay(l, b):
        for x in others_x:
            across(l, b, x * 2 + my_core, x * 2 + my_core).wait_recv()
            inside(l, b, x * 2 + my_core, x).start()

    def mix(l, b):
        if b == 0:
            big[l][7].wait()
        for x in [my_x] + others_x:
            inside(l, b, x * 2 + peer_core, x).wait_recv()
        flat = gated[l, b].reshape(total_rows, heads * size)
        mixed[l, b] = jnp.dot(flat, wout[l], preferred_element_type=F32).astype(BF16)
        for z in others_z[::-1] + [my_z]:
            for y in others_y:
                scatter_y(l, b, z, my_y, y).start()

    def folded(l, b, z):
        total = mixed[l, b, tp_rows(z * n_y + my_y), :].astype(F32)
        for y in others_y:
            scatter_y(l, b, z, y, y).wait_recv()
            total = total + r["mixed_y"][l, b, z, y].astype(F32)
        return total

    def fold(l, b):
        for z in others_z[::-1]:
            r["mixed_s"][l, b, z] = folded(l, b, z).astype(BF16)
            scatter_z(l, b, my_z, z).start()

    def finish(l, b):
        total = folded(l, b, my_z)
        for z in sources_z:
            scatter_z(l, b, z, z).wait_recv()
            total = total + r["mixed_in"][l, b, z].astype(F32)
        result = (current[l, b].astype(F32) + total).astype(BF16)
        if l == LAYERS - 1:
            tokens_out[b] = result
        else:
            current[l + 1, b] = result
            begin(l + 1, b)

    steps = []
    for l in range(LAYERS):
        for b in range(BATCHES):
            base = l * PERIOD + b * LAG
            for j in range(n_z - 1):
                steps.append((base + ISSUE["forward"] * (j + 1), functools.partial(forward, l, b, j)))
            for name, step in (
                ("project", project),
                ("exchange", exchange),
                ("attend", attend),
                ("relay", relay),
                ("mix", mix),
                ("fold", fold),
                ("finish", finish),
            ):
                steps.append((base + ISSUE[name], functools.partial(step, l, b)))
    for _, step in sorted(steps, key=lambda item: item[0]):
        step()

    for l in range(LAYERS):
        max_out[l] = jnp.transpose(top_buf[l])[0:heads, :]
    for l in range(LAYERS):
        for b in range(BATCHES):
            for z in others_z:
                gather_z(l, b, my_z, z).wait_send()
                scatter_z(l, b, my_z, z).wait_send()
                for y in others_y:
                    gather_y(l, b, z, my_y, y).wait_send()
                    scatter_y(l, b, z, my_y, y).wait_send()
            for y in others_y:
                gather_y(l, b, my_z, my_y, y, own=True).wait_send()
                scatter_y(l, b, my_z, my_y, y).wait_send()
            one_gate(l, b).wait_send()
            for c in range(4):
                one_main(l, b, c).wait_send()
            for x in others_x:
                two_gate(l, b, my_x, x).wait_send()
                for c in range(4):
                    two_main(l, b, c, my_x, x).wait_send()
                across(l, b, my_dp, x * 2 + my_core).wait_send()
            for x in [my_x] + others_x:
                inside(l, b, x * 2 + my_core, x).wait_send()


def store(*refs):
    sem = refs[-1]
    copies = [pltpu.make_async_copy(refs[i], refs[4 + i], sem.at[i]) for i in range(4)]
    for copy in copies:
        copy.start()
    for copy in copies:
        copy.wait()


def per_device(
    tokens,
    lengths,
    norm_gain,
    query_weight,
    key_weight,
    value_weight,
    outgate_weight,
    input_gate_weight,
    forget_gate_weight,
    forget_bias,
    out_weight,
    cell_state,
    norm_state,
    max_state,
):
    n_tp, n_dp = lax.axis_size("tp"), lax.axis_size("dp")
    seq_here, span, feat = tokens.shape
    seqs, heads, size = cell_state.shape[1:4]
    own_rows, rows = seq_here * span // BATCHES, seqs * span // BATCHES
    cols, chips = heads * size, n_dp // 2
    everyone, many = n_tp * own_rows, chips * rows
    n_y = chips if n_tp % chips == 0 else 1
    n_z = n_tp // n_y
    vmem = pl.BlockSpec(memory_space=pltpu.VMEM)
    hbm = pl.BlockSpec(memory_space=pltpu.HBM)
    V, sem = pltpu.VMEM, pltpu.SemaphoreType.DMA
    LB = (LAYERS, BATCHES)
    inputs = {
        "tokens": tokens.reshape(BATCHES, own_rows, feat),
        "lengths_in": lengths,
        "gain_in": norm_gain,
        "weight_q": query_weight,
        "weight_k": key_weight,
        "weight_v": value_weight,
        "weight_o": outgate_weight,
        "weight_in": jnp.swapaxes(input_gate_weight, 1, 2),
        "weight_forget": jnp.swapaxes(forget_gate_weight, 1, 2),
        "bias_in": forget_bias,
        "weight_out": out_weight,
        "cell_in": cell_state,
        "norm_in": norm_state,
        "max_in": jnp.swapaxes(max_state, 1, 2),
    }
    outputs = {
        "tokens_out": V((BATCHES, own_rows, feat), BF16),
        "cells": V(cell_state.shape, F32),
        "norm_out": V(norm_state.shape, F32),
        "max_out": V((LAYERS, heads, seqs), F32),
    }
    scratch = {
        "lengths": pltpu.SMEM(lengths.shape, jnp.int32),
        "gain": V(norm_gain.shape, F32),
        "norm": V(norm_state.shape, F32),
        "stabils": V((LAYERS, heads, seqs), F32),
        "bias": V(forget_bias.shape, F32),
        "current": V((*LB, own_rows, feat), BF16),
        "wts": V((LAYERS, 4, feat, cols), BF16),
        "wgate": V((LAYERS, 2, input_gate_weight.shape[2], feat), BF16),
        "wout": V((LAYERS, cols, feat), BF16),
        "pad": V((LAYERS, seqs + 8, LANES), F32),
        "top_buf": V((LAYERS, seqs, LANES), F32),
        "gate_w": V((LAYERS, LANES, feat), BF16),
        "gathered": V((*LB, everyone, feat), BF16),
        "scaled": V((2, many, feat), BF16),
        "both": V((2, many, cols), F32),
        "own_main": V((BATCHES, 4, many, cols), F32),
        "own_gate": V((BATCHES, 2, many, LANES), F32),
        "send1": V((*LB, 4, many, cols), BF16),
        "send1g": V((*LB, many, LANES), BF16),
        "recv1": V((*LB, 4, many, cols), BF16),
        "recv1g": V((*LB, many, LANES), BF16),
        "send2": V((*LB, 4, many, cols), BF16),
        "send2g": V((*LB, many, LANES), BF16),
        "recv2": V((*LB, 4, chips, rows, cols), BF16),
        "recv2g": V((*LB, chips, rows, LANES), BF16),
        "heads_buf": V((BATCHES, 4, rows, cols), BF16),
        "gated": V((*LB, n_dp, rows, cols), BF16),
        "mixed": V((*LB, everyone, feat), BF16),
        "mixed_s": V((*LB, n_z, own_rows, feat), BF16),
        "mixed_y": V((*LB, n_z, n_y, own_rows, feat), BF16),
        "mixed_in": V((*LB, n_z, own_rows, feat), BF16),
        "load_sem": sem((6 + 8 * LAYERS,)),
        "gat_s": sem((*LB, n_z)),
        "gat_r": sem((*LB, n_z)),
        "gfw_s": sem((*LB, n_z, n_y)),
        "gfw_r": sem((*LB, n_z, n_y)),
        "one_s": sem((*LB, 5)),
        "one_r": sem((*LB, 5)),
        "two_s": sem((*LB, 5, chips)),
        "two_r": sem((*LB, 5, chips)),
        "gg_s": sem((*LB, chips)),
        "gg_r": sem((*LB, chips)),
        "fw_s": sem((*LB, chips)),
        "fw_r": sem((*LB, chips)),
        "mix_s": sem((*LB, n_z)),
        "mix_r": sem((*LB, n_z)),
        "my_s": sem((*LB, n_z, n_y)),
        "my_r": sem((*LB, n_z, n_y)),
    }
    names = (*inputs, *outputs, *scratch)
    result = pl.pallas_call(
        functools.partial(kernel, (n_tp, n_dp, span, heads, size, n_y, names)),
        out_shape=tuple(outputs.values()),
        in_specs=[hbm] * len(inputs),
        out_specs=(vmem,) * len(outputs),
        scratch_shapes=list(scratch.values()),
        compiler_params=pltpu.CompilerParams(
            collective_id=0, has_side_effects=True, vmem_limit_bytes=56 * 1024 * 1024
        ),
    )(*inputs.values())
    result = pl.pallas_call(
        store,
        out_shape=tuple(jax.ShapeDtypeStruct(part.shape, part.dtype) for part in result),
        in_specs=[vmem] * 4,
        out_specs=(pl.BlockSpec(memory_space=pl.ANY),) * 4,
        scratch_shapes=[sem((4,))],
        compiler_params=pltpu.CompilerParams(vmem_limit_bytes=16 * 1024 * 1024),
    )(*result)
    return (result[0].reshape(tokens.shape), *result[1:3], jnp.swapaxes(result[3], 1, 2))


def solution(mesh):
    return jax.shard_map(
        per_device,
        mesh=mesh,
        in_specs=(
            P("tp", None, "dp"),
            P("dp"),
            P(None, "dp"),
            P(None, "dp", "tp"),
            P(None, "dp", "tp"),
            P(None, "dp", "tp"),
            P(None, "dp", "tp"),
            P(),
            P(),
            P(None, "tp"),
            P(None, "tp", "dp"),
            P(None, "dp", "tp", None, None),
            P(None, "dp", "tp", None),
            P(None, "dp", "tp"),
        ),
        out_specs=(
            P("tp", None, "dp"),
            P(None, "dp", "tp", None, None),
            P(None, "dp", "tp", None),
            P(None, "dp", "tp"),
        ),
        check_vma=False,
    )
```

```python
import functools
import types
import jax
import jax.numpy as jnp
from jax import lax
from jax.experimental import pallas as pl
from jax.experimental.pallas import tpu as pltpu
from jax.sharding import PartitionSpec as P

EPSILON = 1e-06
NEG_FILL = -1e30
LANES = 128
HIGH = lax.Precision.HIGHEST
BF16 = jnp.bfloat16
F32 = jnp.float32
MESH = pl.DeviceIdType.MESH
BATCHES = 4
LAYERS = 2
AHEAD = 2
FORWARD, PROJECT, EXCHANGE, ATTEND, UPDATE, RELAY, MIX, FOLD, FINISH = range(9)
ORDER = (
    0, 1, 2, 100, 101, 102, 10, 200, 201, 20, 110, 202, 300, 301, 302, 120,
    30, 210, 50, 130, 60, 220, 310, 70, 150, 71, 320, 160, 230, 72, 170, 330,
    250, 171, 80, 260, 172, 340, 350, 270, 1000, 360, 271, 272, 1001, 40, 1002, 180,
    1100, 370, 1101, 371, 372, 1102, 280, 1010, 380, 1020, 1200, 1110, 1201, 140, 1202, 240,
    1120, 1030, 1300, 1301, 1302, 1210, 1050, 1130, 1060, 1220, 1310, 1150, 1320, 1070, 1230, 1160,
    1071, 1040, 1330, 1250, 1072, 1170, 1171, 1260, 1172, 1140, 1350, 1080, 1360, 1270, 1340, 1271,
    1180, 1272, 1370, 1240, 1371, 1280, 1372, 1380,
)


def plan(n_z):
    result = []
    for entry in ORDER:
        l, b, step, third = entry // 1000, entry // 100 % 10, entry // 10 % 10, entry % 10
        if step in (FORWARD, FOLD):
            count = n_z - 1
            result += [(l, b, step, j) for j in range(third * count // 3, (third + 1) * count // 3)]
        else:
            result.append((l, b, step, 0))
    return result


def pack_squares(block):
    lane = lax.broadcasted_iota(jnp.int32, block.shape, 1)
    square = jnp.sum(jnp.where(lane >= LANES - 3, block, 0.0), axis=1, keepdims=True)
    first = square.astype(BF16).astype(F32)
    rest = square - first
    second = rest.astype(BF16).astype(F32)
    third = rest - second
    block = jnp.where(lane == LANES - 3, first, block)
    block = jnp.where(lane == LANES - 2, second, block)
    return jnp.where(lane == LANES - 1, third, block).astype(BF16)


def flip_bits(value, mask):
    result = value
    bit = 1
    while bit <= mask:
        if mask & bit:
            result = result + bit * (1 - 2 * lax.rem(value // bit, 2))
        bit = bit * 2
    return result


def kernel(sizes, *refs):
    n_tp, n_dp, span, heads, size, n_y, names = sizes
    r = types.SimpleNamespace(**dict(zip(names, refs)))
    lengths, norm, stabils, gain = r.lengths, r.norm, r.stabils, r.gain
    cells, norm_out, max_out, tokens_out = r.cells, r.norm_out, r.max_out, r.tokens_out
    current, wts, wgate, wout = r.current, r.wts, r.wgate, r.wout
    gathered, scaled, gate_w, both = r.gathered, r.scaled, r.gate_w, r.both
    own_gate, own_main, heads_buf = r.own_gate, r.own_main, r.heads_buf
    gated, mixed, top_buf, pad = r.gated, r.mixed, r.top_buf, r.pad
    load_sem = r.load_sem
    chips = n_dp // 2
    n_z = n_tp // n_y
    my_tp, my_dp = lax.axis_index("tp"), lax.axis_index("dp")
    my_x, my_core = my_dp // 2, lax.rem(my_dp, 2)
    peer_core = 1 - my_core
    peer = my_x * 2 + peer_core
    my_z, my_y = my_tp // n_y, lax.rem(my_tp, n_y)
    own_rows, feat = current.shape[2:]
    seqs = cells.shape[1]
    own_part = own_rows // span
    own_seqs = own_part * BATCHES
    ratio = seqs // own_seqs
    seqs_b = seqs // BATCHES
    rows = seqs_b * span
    total_rows = n_dp * rows
    key_scale = size ** (-0.5)

    def load(index, source, target):
        return pltpu.make_async_copy(source, target, load_sem.at[index])

    start = pl.multiple_of(my_dp * feat, feat)
    small = [
        load(0, r.tokens, current.at[0]),
        load(1, r.lengths_in, lengths),
        load(2, r.gain_in, gain),
        load(3, r.norm_in, norm),
        load(4, r.max_in, stabils),
        load(5, r.bias_in, r.bias),
    ]
    big = []
    for l in range(LAYERS):
        part = []
        for i, source in enumerate((r.weight_in, r.weight_forget)):
            part.append(load(6 + 4 * l, source.at[l, :, pl.ds(start, feat)], wgate.at[l, i]))
        for i, source in enumerate((r.weight_q, r.weight_k, r.weight_v, r.weight_o)):
            part.append(load(7 + 4 * l, source.at[l], wts.at[l, i]))
        part.append(load(8 + 4 * l, r.cell_in.at[l], cells.at[l]))
        part.append(load(9 + 4 * l, r.weight_out.at[l], wout.at[l]))
        big.append(part)
    for copy in small + big[0] + big[1]:
        copy.start()

    power = n_z & (n_z - 1) == 0
    peers_y = [(lax.rem(my_y + j, n_y), j - 1, n_y - j - 1) for j in range(1, n_y)]
    peers_x = [(lax.rem(my_x + j, chips), j - 1, chips - j - 1) for j in range(1, chips)]
    if power:
        peers_z = [(flip_bits(my_z, j), j - 1, j - 1) for j in range(1, n_z)]
    else:
        peers_z = [(lax.rem(my_z + j, n_z), j - 1, n_z - j - 1) for j in range(1, n_z)]
    barrier = pltpu.get_barrier_semaphore()
    for y, _, _ in peers_y:
        pl.semaphore_signal(
            barrier, inc=1, device_id={"tp": my_z * n_y + y}, device_id_type=MESH
        )
    for z, _, _ in peers_z:
        pl.semaphore_signal(
            barrier, inc=1, device_id={"tp": z * n_y + my_y}, device_id_type=MESH
        )
    for x, _, _ in peers_x:
        pl.semaphore_signal(
            barrier, inc=1, device_id={"dp": x * 2 + my_core}, device_id_type=MESH
        )
    pl.semaphore_signal(barrier, inc=1, device_id={"dp": peer}, device_id_type=MESH)
    pl.semaphore_wait(barrier, len(peers_y) + len(peers_z) + chips)

    def remote(src, dst, s, rcv, where):
        return pltpu.make_async_remote_copy(
            src_ref=src, dst_ref=dst, send_sem=s, recv_sem=rcv, device_id=where, device_id_type=MESH
        )

    def tp_rows(t):
        return pl.ds(pl.multiple_of(t * own_rows, own_rows), own_rows)

    def x_rows(x):
        return pl.ds(pl.multiple_of(x * rows, rows), rows)

    def drain_sent(ref, sem_ref):
        remote(ref, ref, sem_ref, sem_ref, {"dp": peer}).wait_send()

    def drain_received(ref, sem_ref):
        remote(ref, ref, sem_ref, sem_ref, {"dp": peer}).wait_recv()

    def block_rows(count):
        return pl.ds(0, count * own_rows)

    def gather_z(l, b, peer_z, own=True):
        z, here, there = peer_z
        return remote(
            current.at[l, b],
            gathered.at[l, b, tp_rows((my_z if own else z) * n_y + my_y)],
            r.gat_s.at[b],
            r.gat_r.at[b, there if own else here],
            {"tp": z * n_y + my_y},
        )

    def gather_y(l, b, z, peer_y, own):
        part = gathered.at[l, b, tp_rows(z * n_y + my_y)]
        return remote(
            current.at[l, b] if own else part,
            part,
            r.gat_s.at[b] if own else r.gfw_s.at[b],
            r.gfw_r.at[b],
            {"tp": my_z * n_y + peer_y[0]},
        )

    def one_gate(l, b):
        return remote(
            r.send1g.at[l, b],
            r.recv1g.at[l, b],
            r.one_s.at[b, 1],
            r.one_r.at[b, 4],
            {"dp": peer},
        )

    def one_main(l, b, c):
        return remote(
            r.send1.at[l, b, c],
            r.recv1.at[l, b, c],
            r.one_s.at[b, 0],
            r.one_r.at[b, c],
            {"dp": peer},
        )

    def two_gate(l, b, peer_x):
        x, _, there = peer_x
        return remote(
            r.send2g.at[l, b, x_rows(x)],
            r.recv2g.at[l, b, there],
            r.two_s.at[b, 1],
            r.two_r.at[b, 1],
            {"dp": x * 2 + my_core},
        )

    def two_main(l, b, c, peer_x):
        x, _, there = peer_x
        return remote(
            r.send2.at[l, b, c, x_rows(x)],
            r.recv2.at[l, b, c, there],
            r.two_s.at[b, 0],
            r.two_r.at[b, 0],
            {"dp": x * 2 + my_core},
        )

    def across(l, b, peer_x, own=True):
        x, here, there = peer_x
        part = gated.at[l, b, my_dp if own else x * 2 + my_core]
        return remote(
            part,
            part,
            r.gg_s.at[b],
            r.gg_r.at[b, there if own else here],
            {"dp": x * 2 + my_core},
        )

    def inside(l, b, block):
        part = gated.at[l, b, block]
        return remote(part, part, r.fw_s.at[b], r.fw_r.at[b], {"dp": peer})

    def scatter_y(l, b, z, peer_y):
        y, _, there = peer_y
        return remote(
            mixed.at[l, b, tp_rows(z * n_y + y)],
            r.mixed_y.at[l, b, z, there],
            r.my_s.at[b],
            r.my_r.at[b, z],
            {"tp": my_z * n_y + y},
        )

    def scatter_z(l, b, peer_z):
        z, here, there = peer_z
        return remote(
            r.mixed_s.at[l, b, here],
            r.mixed_in.at[l, b, there],
            r.mix_s.at[b],
            r.mix_r.at[b],
            {"tp": z * n_y + my_y},
        )

    def sent_gather(l, b):
        drain_sent(gathered.at[l, b, block_rows(n_z + n_y - 2)], r.gat_s.at[b])
        drain_sent(gathered.at[l, b, block_rows((n_z - 1) * (n_y - 1))], r.gfw_s.at[b])

    def sent_project(l, b):
        drain_sent(r.send1.at[l, b], r.one_s.at[b, 0])
        drain_sent(r.send1g.at[l, b], r.one_s.at[b, 1])
        drain_sent(r.recv2.at[l, b], r.two_s.at[b, 0])
        drain_sent(r.recv2g.at[l, b], r.two_s.at[b, 1])

    def sent_attend(l, b):
        drain_sent(gated.at[l, b, pl.ds(0, chips - 1)], r.gg_s.at[b])
        drain_sent(gated.at[l, b, pl.ds(0, chips)], r.fw_s.at[b])

    def sent_mix(l, b):
        drain_sent(r.mixed_y.at[l, b], r.my_s.at[b])
        drain_sent(r.mixed_s.at[l, b], r.mix_s.at[b])

    def begin(l, b):
        if l:
            sent_gather(l - 1, b)
        for peer_z in peers_z:
            gather_z(l, b, peer_z).start()
        for peer_y in peers_y:
            gather_y(l, b, my_z, peer_y, own=True).start()
        gathered[l, b, tp_rows(my_tp)] = current[l, b]

    small[0].wait()
    for b in range(BATCHES):
        begin(0, b)
    for copy in small[1:]:
        copy.wait()

    row_id = lax.broadcasted_iota(jnp.int32, (rows, rows), 0)
    col_id = lax.broadcasted_iota(jnp.int32, (rows, rows), 1)
    allowed = (row_id // span == col_id // span) & (col_id <= row_id)
    lane = lax.broadcasted_iota(jnp.int32, (rows, LANES), 1)
    row_l = lax.broadcasted_iota(jnp.int32, (rows, LANES), 0)
    runs = [
        [slice(j * own_seqs + b * own_part, j * own_seqs + (b + 1) * own_part) for j in range(ratio)]
        for b in range(BATCHES)
    ]

    def live_of(b):
        reach = jnp.zeros((rows, LANES), jnp.int32)
        place = 0
        for run in runs[b]:
            for s in range(run.start, run.stop):
                reach = jnp.where(row_l // span == place, lengths[s], reach)
                place = place + 1
        return lax.rem(row_l, span) < reach

    pad[...] = jnp.zeros_like(pad)
    for l in range(LAYERS):
        pad[l, 0:seqs, 0:heads] = jnp.transpose(stabils[l])
        pad[l, seqs : seqs + 1, 0:heads] = r.bias[l : l + 1, :]

    def spread(value):
        wide = jnp.broadcast_to(value[:, None, :], (seqs_b, span, value.shape[-1]))
        return wide.reshape(rows, value.shape[-1])

    def last(value):
        return value.reshape(seqs_b, span, value.shape[-1])[:, span - 1, :]

    arrived = set()

    def arrive(l, first, end):
        if (l, first) not in arrived:
            arrived.add((l, first))
            if end == first + 1:
                big[l][first].wait()
            else:
                whole = wgate.at[l] if first == 0 else wts.at[l]
                load(6 + 4 * l + (first > 0), whole, whole).wait()

    def gate_columns(l):
        arrive(l, 0, 2)
        total_heads = wgate.shape[2]
        pick_r = lax.broadcasted_iota(jnp.int32, (LANES, total_heads), 1)
        pick_c = lax.broadcasted_iota(jnp.int32, (LANES, total_heads), 0)
        head_start = my_tp * heads
        pick_in = ((pick_r == head_start + pick_c) & (pick_c < heads)).astype(F32).astype(BF16)
        pick_fg = (
            ((pick_r == head_start + pick_c - heads) & (pick_c >= heads) & (pick_c < 2 * heads))
            .astype(F32)
            .astype(BF16)
        )
        gate_w[l] = (
            jnp.dot(pick_in, wgate[l, 0], preferred_element_type=F32)
            + jnp.dot(pick_fg, wgate[l, 1], preferred_element_type=F32)
        ).astype(BF16)

    for l in range(LAYERS):
        gate_columns(l)

    def forward(l, b, j):
        gather_z(l, b, peers_z[j], own=False).wait_recv()
        for peer_y in peers_y:
            gather_y(l, b, peers_z[j][0], peer_y, own=False).start()

    def project(l, b):
        if l:
            sent_project(l - 1, b)
        drain_received(gathered.at[l, b, block_rows(n_z * (n_y - 1))], r.gfw_r.at[b])
        gain_row = gain[l : l + 1, :]
        for d in range(n_dp):
            block = gathered[l, b, d * rows : (d + 1) * rows].astype(F32)
            core, x = d % 2, d // 2
            scaled[core, x * rows : (x + 1) * rows] = (block * gain_row).astype(BF16)
            own_gate[b, core, x * rows : (x + 1) * rows] = jnp.broadcast_to(
                jnp.sum(block * block, axis=1, keepdims=True), (rows, LANES)
            )
        lane_all = lax.broadcasted_iota(jnp.int32, (chips * rows, LANES), 1)
        for core in range(2):
            part = lax.dot_general(
                scaled[core], gate_w[l], (((1,), (1,)), ((), ())), preferred_element_type=F32
            )
            own_gate[b, core] = jnp.where(lane_all == LANES - 3, own_gate[b, core], part)
        r.send1g[l, b] = pack_squares(own_gate[b, peer_core])
        one_gate(l, b).start()
        arrive(l, 2, 6)

        def one(c, carry):
            flat = scaled[...].reshape(2 * chips * rows, feat)
            both[...] = jnp.dot(flat, wts[l, c], preferred_element_type=F32).reshape(both.shape)
            r.send1[l, b, c] = both[peer_core].astype(BF16)
            one_main(l, b, c).start()
            own_main[b, c] = both[my_core]

            @pl.when(c == AHEAD)
            def _():
                exchange_gate(l, b)

            @pl.when(c >= AHEAD)
            def _():
                exchange_main(l, b, c - AHEAD)

            return carry

        lax.fori_loop(0, 4, one, 0)

    def exchange_gate(l, b):
        one_gate(l, b).wait_recv()
        summed = own_gate[b, my_core] + r.recv1g[l, b].astype(F32)
        own_gate[b, my_core] = summed
        r.send2g[l, b] = pack_squares(summed)
        for peer_x in peers_x:
            two_gate(l, b, peer_x).start()

    def exchange_main(l, b, c):
        one_main(l, b, c).wait_recv()
        own = own_main[b, c] + r.recv1[l, b, c].astype(F32)
        own_main[b, c] = own
        r.send2[l, b, c] = own.astype(BF16)
        for peer_x in peers_x:
            two_main(l, b, c, peer_x).start()

    def exchange(l, b):
        def one(c, carry):
            exchange_main(l, b, c)
            return carry

        lax.fori_loop(4 - AHEAD, 4, one, 0)

    kept = {}

    def attend(l, b):
        live = live_of(b)
        if l:
            sent_attend(l - 1, b)
        drain_received(r.recv2g.at[l, b], r.two_r.at[b, 1])
        sums = own_gate[b, my_core, x_rows(my_x)]
        for j in range(chips - 1):
            sums = sums + r.recv2g[l, b, j].astype(F32)
        square = jnp.sum(jnp.where(lane >= LANES - 3, sums, 0.0), axis=1, keepdims=True)
        scale = lax.rsqrt(square / (feat * n_dp) + EPSILON)
        gates = scale * sums
        stabil = jnp.concatenate([pad[l, run] for run in runs[b]], axis=0)
        forget = pltpu.roll(gates, LANES - heads, 1) + pad[l, seqs : seqs + 1, :]
        log_forget = jnp.minimum(forget, 0.0) - jnp.log1p(jnp.exp(-jnp.abs(forget)))
        in_gate = jnp.where(live, gates, NEG_FILL)
        log_forget = jnp.where(live, log_forget, 0.0)
        cumul = jnp.dot(
            allowed.astype(F32), log_forget, preferred_element_type=F32, precision=HIGH
        )
        carried = cumul + spread(stabil)
        source = jnp.transpose(in_gate - cumul)
        arrive(l, 6, 7)
        drain_received(r.recv2.at[l, b], r.two_r.at[b, 0])
        for c in range(4):
            full = own_main[b, c, x_rows(my_x)]
            for j in range(chips - 1):
                full = full + r.recv2[l, b, c, j].astype(F32)
            heads_buf[l, b, c] = (scale * full).astype(BF16)

        ids = [s for run in runs[b] for s in range(run.start, run.stop)]
        running = jnp.zeros((rows, LANES), F32)
        for h in range(heads):
            span_h = slice(h * size, (h + 1) * size)
            normer = jnp.concatenate([norm[l, run, h, :] for run in runs[b]], axis=0)
            q, k, v = (heads_buf[l, b, c, :, span_h] for c in range(3))
            weight = jnp.where(allowed, cumul[:, h : h + 1] + source[h : h + 1, :], NEG_FILL)
            top = jnp.maximum(jnp.max(weight, axis=1, keepdims=True), carried[:, h : h + 1])
            running = jnp.where(lane == h, top, running)
            decay = jnp.exp(carried[:, h : h + 1] - top)
            scores = lax.dot_general(
                q, k, (((1,), (1,)), ((), ())), preferred_element_type=F32
            )
            scores = scores * key_scale * jnp.exp(weight - top)
            numer = jnp.dot(scores.astype(BF16), v, preferred_element_type=F32)
            from_cell = jnp.concatenate(
                [
                    jnp.dot(
                        q[i * span : (i + 1) * span],
                        cells[l, s, h].astype(BF16),
                        preferred_element_type=F32,
                    )
                    for i, s in enumerate(ids)
                ],
                axis=0,
            )
            numer = numer + decay * from_cell
            from_norm = jnp.sum(q.astype(F32) * spread(normer), axis=1, keepdims=True)
            denom = jnp.sum(scores, axis=1, keepdims=True) + decay * from_norm
            readout = numer / jnp.maximum(jnp.abs(denom), 1.0)
            readout = jnp.where(live, readout, 0.0)
            outgate = heads_buf[l, b, 3, :, span_h].astype(F32)
            gated[l, b, my_dp, :, span_h] = (readout / (1.0 + jnp.exp(-outgate))).astype(BF16)

        for peer_x in peers_x:
            across(l, b, peer_x).start()
        inside(l, b, my_dp).start()
        kept[l, b] = running, cumul, in_gate, stabil

    def update(l, b):
        running, cumul, in_gate, stabil = kept[l, b]
        ids = [s for run in runs[b] for s in range(run.start, run.stop)]
        top_last, cumul_last = last(running), last(cumul)
        weights = jnp.exp(spread(cumul_last - top_last) - cumul + in_gate)
        fade = jnp.exp(cumul_last + stabil - top_last)
        for j, run in enumerate(runs[b]):
            top_buf[l, run] = top_last[j * own_part : (j + 1) * own_part]
        seq_col = lax.broadcasted_iota(jnp.int32, (size, rows), 1) // span
        pick = (
            lax.broadcasted_iota(jnp.int32, (seqs_b, rows), 1) // span
            == lax.broadcasted_iota(jnp.int32, (seqs_b, rows), 0)
        ).astype(F32)
        for h in range(heads):
            span_h = slice(h * size, (h + 1) * size)
            normer = jnp.concatenate([norm[l, run, h, :] for run in runs[b]], axis=0)
            v = heads_buf[l, b, 2, :, span_h]
            k = heads_buf[l, b, 1, :, span_h].astype(F32) * key_scale * weights[:, h : h + 1]
            flipped = jnp.transpose(k)
            stacked = jnp.concatenate(
                [jnp.where(seq_col == i, flipped, 0.0).astype(BF16) for i in range(seqs_b)], axis=0
            )
            added = jnp.dot(stacked, v, preferred_element_type=F32)
            for i, s in enumerate(ids):
                cells[l, s, h] = (
                    fade[i : i + 1, h : h + 1] * cells[l, s, h]
                    + added[i * size : (i + 1) * size]
                )
            moved = fade[:, h : h + 1] * normer + jnp.dot(
                pick, k, preferred_element_type=F32, precision=HIGH
            )
            for j, run in enumerate(runs[b]):
                norm_out[l, run, h, :] = moved[j * own_part : (j + 1) * own_part]

    def relay(l, b):
        for peer_x in peers_x:
            across(l, b, peer_x, own=False).wait_recv()
            inside(l, b, peer_x[0] * 2 + my_core).start()

    def mix(l, b):
        arrive(l, 7, 8)
        if l:
            sent_mix(l - 1, b)
        drain_received(gated.at[l, b, pl.ds(0, chips)], r.fw_r.at[b])
        flat = gated[l, b].reshape(total_rows, heads * size)
        mixed[l, b] = jnp.dot(flat, wout[l], preferred_element_type=F32).astype(BF16)
        for z in [peer_z[0] for peer_z in peers_z[::-1]] + [my_z]:
            for peer_y in peers_y:
                scatter_y(l, b, z, peer_y).start()

    def folded(l, b, z):
        total = mixed[l, b, tp_rows(z * n_y + my_y), :].astype(F32)
        drain_received(r.mixed_y.at[l, b, z], r.my_r.at[b, z])
        for j in range(n_y - 1):
            total = total + r.mixed_y[l, b, z, j].astype(F32)
        return total

    def fold(l, b, j):
        peer_z = peers_z[::-1][j]
        r.mixed_s[l, b, peer_z[1]] = folded(l, b, peer_z[0]).astype(BF16)
        scatter_z(l, b, peer_z).start()

    def finish(l, b):
        total = folded(l, b, my_z)
        drain_received(r.mixed_in.at[l, b], r.mix_r.at[b])
        for j in range(n_z - 1):
            total = total + r.mixed_in[l, b, j].astype(F32)
        result = (current[l, b].astype(F32) + total).astype(BF16)
        if l == LAYERS - 1:
            tokens_out[b] = result
        else:
            current[l + 1, b] = result
            begin(l + 1, b)

    steps = (forward, project, exchange, attend, update, relay, mix, fold, finish)
    for l, b, step, j in plan(n_z):
        if step in (FORWARD, FOLD):
            steps[step](l, b, j)
        else:
            steps[step](l, b)

    for l in range(LAYERS):
        max_out[l] = jnp.transpose(top_buf[l])[0:heads, :]
    for b in range(BATCHES):
        for sent in (sent_gather, sent_project, sent_attend, sent_mix):
            sent(LAYERS - 1, b)


def store(*refs):
    sem = refs[-1]
    copies = [pltpu.make_async_copy(refs[i], refs[4 + i], sem.at[i]) for i in range(4)]
    for copy in copies:
        copy.start()
    for copy in copies:
        copy.wait()


def per_device(
    tokens,
    lengths,
    norm_gain,
    query_weight,
    key_weight,
    value_weight,
    outgate_weight,
    input_gate_weight,
    forget_gate_weight,
    forget_bias,
    out_weight,
    cell_state,
    norm_state,
    max_state,
):
    n_tp, n_dp = lax.axis_size("tp"), lax.axis_size("dp")
    seq_here, span, feat = tokens.shape
    seqs, heads, size = cell_state.shape[1:4]
    own_rows, rows = seq_here * span // BATCHES, seqs * span // BATCHES
    cols, chips = heads * size, n_dp // 2
    everyone, many = n_tp * own_rows, chips * rows
    n_y = chips if n_tp % chips == 0 else 1
    n_z = n_tp // n_y
    vmem = pl.BlockSpec(memory_space=pltpu.VMEM)
    hbm = pl.BlockSpec(memory_space=pltpu.HBM)
    V, sem = pltpu.VMEM, pltpu.SemaphoreType.DMA
    LB = (LAYERS, BATCHES)
    inputs = dict(
        tokens=tokens.reshape(BATCHES, own_rows, feat),
        lengths_in=lengths,
        gain_in=norm_gain,
        weight_q=query_weight,
        weight_k=key_weight,
        weight_v=value_weight,
        weight_o=outgate_weight,
        weight_in=jnp.swapaxes(input_gate_weight, 1, 2),
        weight_forget=jnp.swapaxes(forget_gate_weight, 1, 2),
        bias_in=forget_bias,
        weight_out=out_weight,
        cell_in=cell_state,
        norm_in=norm_state,
        max_in=jnp.swapaxes(max_state, 1, 2),
    )
    outputs = dict(
        tokens_out=V((BATCHES, own_rows, feat), BF16),
        cells=V(cell_state.shape, F32),
        norm_out=V(norm_state.shape, F32),
        max_out=V((LAYERS, heads, seqs), F32),
    )
    scratch = dict(
        lengths=pltpu.SMEM(lengths.shape, jnp.int32),
        gain=V(norm_gain.shape, F32),
        norm=V(norm_state.shape, F32),
        stabils=V((LAYERS, heads, seqs), F32),
        bias=V(forget_bias.shape, F32),
        current=V((*LB, own_rows, feat), BF16),
        wts=V((LAYERS, 4, feat, cols), BF16),
        wgate=V((LAYERS, 2, input_gate_weight.shape[2], feat), BF16),
        wout=V((LAYERS, cols, feat), BF16),
        pad=V((LAYERS, seqs + 8, LANES), F32),
        top_buf=V((LAYERS, seqs, LANES), F32),
        gate_w=V((LAYERS, LANES, feat), BF16),
        gathered=V((*LB, everyone, feat), BF16),
        scaled=V((2, many, feat), BF16),
        both=V((2, many, cols), F32),
        own_main=V((BATCHES, 4, many, cols), F32),
        own_gate=V((BATCHES, 2, many, LANES), F32),
        send1=V((*LB, 4, many, cols), BF16),
        send1g=V((*LB, many, LANES), BF16),
        recv1=V((*LB, 4, many, cols), BF16),
        recv1g=V((*LB, many, LANES), BF16),
        send2=V((*LB, 4, many, cols), BF16),
        send2g=V((*LB, many, LANES), BF16),
        recv2=V((*LB, 4, chips - 1, rows, cols), BF16),
        recv2g=V((*LB, chips - 1, rows, LANES), BF16),
        heads_buf=V((*LB, 4, rows, cols), BF16),
        gated=V((*LB, n_dp, rows, cols), BF16),
        mixed=V((*LB, everyone, feat), BF16),
        mixed_s=V((*LB, n_z - 1, own_rows, feat), BF16),
        mixed_y=V((*LB, n_z, n_y - 1, own_rows, feat), BF16),
        mixed_in=V((*LB, n_z - 1, own_rows, feat), BF16),
        load_sem=sem((6 + 4 * LAYERS,)),
        gat_s=sem((BATCHES,)),
        gat_r=sem((BATCHES, n_z - 1)),
        gfw_s=sem((BATCHES,)),
        gfw_r=sem((BATCHES,)),
        one_s=sem((BATCHES, 2)),
        one_r=sem((BATCHES, 5)),
        two_s=sem((BATCHES, 2)),
        two_r=sem((BATCHES, 2)),
        gg_s=sem((BATCHES,)),
        gg_r=sem((BATCHES, chips - 1)),
        fw_s=sem((BATCHES,)),
        fw_r=sem((BATCHES,)),
        mix_s=sem((BATCHES,)),
        mix_r=sem((BATCHES,)),
        my_s=sem((BATCHES,)),
        my_r=sem((BATCHES, n_z)),
    )
    names = (*inputs, *outputs, *scratch)
    result = pl.pallas_call(
        functools.partial(kernel, (n_tp, n_dp, span, heads, size, n_y, names)),
        out_shape=tuple(outputs.values()),
        in_specs=[hbm] * len(inputs),
        out_specs=(vmem,) * len(outputs),
        scratch_shapes=list(scratch.values()),
        compiler_params=pltpu.CompilerParams(
            collective_id=0, has_side_effects=True, vmem_limit_bytes=56 * 1024 * 1024
        ),
    )(*inputs.values())
    result = pl.pallas_call(
        store,
        out_shape=tuple(jax.ShapeDtypeStruct(part.shape, part.dtype) for part in result),
        in_specs=[vmem] * 4,
        out_specs=(pl.BlockSpec(memory_space=pl.ANY),) * 4,
        scratch_shapes=[sem((4,))],
        compiler_params=pltpu.CompilerParams(vmem_limit_bytes=16 * 1024 * 1024),
    )(*result)
    return (result[0].reshape(tokens.shape), *result[1:3], jnp.swapaxes(result[3], 1, 2))


def solution(mesh):
    return jax.shard_map(
        per_device,
        mesh=mesh,
        in_specs=(
            P("tp", None, "dp"),
            P("dp"),
            P(None, "dp"),
            P(None, "dp", "tp"),
            P(None, "dp", "tp"),
            P(None, "dp", "tp"),
            P(None, "dp", "tp"),
            P(),
            P(),
            P(None, "tp"),
            P(None, "tp", "dp"),
            P(None, "dp", "tp", None, None),
            P(None, "dp", "tp", None),
            P(None, "dp", "tp"),
        ),
        out_specs=(
            P("tp", None, "dp"),
            P(None, "dp", "tp", None, None),
            P(None, "dp", "tp", None),
            P(None, "dp", "tp"),
        ),
        check_vma=False,
    )
```

```python
import functools
import types
import jax
import jax.numpy as jnp
from jax import lax
from jax.experimental import pallas as pl
from jax.experimental.pallas import tpu as pltpu
from jax.sharding import PartitionSpec as P

EPSILON = 1e-06
NEG_FILL = -1e30
LANES = 128
HIGH = lax.Precision.HIGHEST
BF16 = jnp.bfloat16
F32 = jnp.float32
MESH = pl.DeviceIdType.MESH
BATCHES = 4
LAYERS = 2
AHEAD = 2
FORWARD, PROJECT, EXCHANGE, ATTEND, UPDATE, RELAY, MIX, FOLD, FINISH, GATES = range(10)
ORDER = (
    0, 1, 2, 100, 101, 102, 10, 200, 20, 201, 110, 202, 90, 300, 120, 301,
    302, 30, 190, 210, 50, 130, 220, 60, 310, 150, 290, 70, 40, 320, 71, 160,
    72, 230, 170, 171, 390, 250, 80, 260, 330, 172, 270, 1000, 350, 271, 360, 272,
    1001, 1002, 180, 1100, 370, 371, 372, 280, 1101, 1102, 1010, 1020, 380, 1200, 1110, 1201,
    1202, 1090, 1300, 1120, 1190, 1030, 1301, 1302, 1210, 1130, 1050, 1220, 1310, 1060, 1320, 1150,
    1290, 1230, 1160, 1390, 1070, 1071, 1240, 1330, 1250, 1170, 1140, 1260, 1040, 1171, 340, 1172,
    1350, 1072, 1360, 1270, 1340, 1271, 1180, 1272, 1370, 1080, 1371, 1280, 1372, 240, 140, 1380,
)


def plan(n_z):
    result = []
    for entry in ORDER:
        l, b, step, third = entry // 1000, entry // 100 % 10, entry // 10 % 10, entry % 10
        if step in (FORWARD, FOLD):
            count = n_z - 1
            result += [(l, b, step, j) for j in range(third * count // 3, (third + 1) * count // 3)]
        else:
            result.append((l, b, step, 0))
    return result


def pack_squares(block):
    lane = lax.broadcasted_iota(jnp.int32, block.shape, 1)
    square = jnp.sum(jnp.where(lane >= LANES - 3, block, 0.0), axis=1, keepdims=True)
    first = square.astype(BF16).astype(F32)
    rest = square - first
    second = rest.astype(BF16).astype(F32)
    third = rest - second
    block = jnp.where(lane == LANES - 3, first, block)
    block = jnp.where(lane == LANES - 2, second, block)
    return jnp.where(lane == LANES - 1, third, block).astype(BF16)


def flip_bits(value, mask):
    result = value
    bit = 1
    while bit <= mask:
        if mask & bit:
            result = result + bit * (1 - 2 * lax.rem(value // bit, 2))
        bit = bit * 2
    return result


def kernel(sizes, *refs):
    n_tp, n_dp, span, heads, size, n_y, names = sizes
    r = types.SimpleNamespace(**dict(zip(names, refs)))
    lengths, norm, stabils, gain = r.lengths, r.norm, r.stabils, r.gain
    cells, norm_out, max_out, tokens_out = r.cells, r.norm_out, r.max_out, r.tokens_out
    current, wts, wgate, wout = r.current, r.wts, r.wgate, r.wout
    gathered, scaled, gate_w = r.gathered, r.scaled, r.gate_w
    own_gate, own_main, heads_buf = r.own_gate, r.own_main, r.heads_buf
    gated, mixed, top_buf, pad = r.gated, r.mixed, r.top_buf, r.pad
    load_sem = r.load_sem
    chips = n_dp // 2
    n_z = n_tp // n_y
    my_tp, my_dp = lax.axis_index("tp"), lax.axis_index("dp")
    my_x, my_core = my_dp // 2, lax.rem(my_dp, 2)
    peer_core = 1 - my_core
    peer = my_x * 2 + peer_core
    my_z, my_y = my_tp // n_y, lax.rem(my_tp, n_y)
    own_rows, feat = current.shape[2:]
    seqs = cells.shape[1]
    own_part = own_rows // span
    own_seqs = own_part * BATCHES
    ratio = seqs // own_seqs
    seqs_b = seqs // BATCHES
    rows = seqs_b * span
    total_rows = n_dp * rows
    key_scale = size ** (-0.5)

    def load(index, source, target):
        return pltpu.make_async_copy(source, target, load_sem.at[index])

    start = pl.multiple_of(my_dp * feat, feat)
    small = [
        load(0, r.tokens, current.at[0]),
        load(1, r.lengths_in, lengths),
        load(2, r.gain_in, gain),
        load(3, r.norm_in, norm),
        load(4, r.max_in, stabils),
        load(5, r.bias_in, r.bias),
    ]
    big = []
    for l in range(LAYERS):
        part = []
        for i, source in enumerate((r.weight_in, r.weight_forget)):
            part.append(load(6 + 4 * l, source.at[l, :, pl.ds(start, feat)], wgate.at[l, i]))
        for i, source in enumerate((r.weight_q, r.weight_k, r.weight_v, r.weight_o)):
            part.append(load(7 + 4 * l, source.at[l], wts.at[l, i]))
        part.append(load(8 + 4 * l, r.cell_in.at[l], cells.at[l]))
        part.append(load(9 + 4 * l, r.weight_out.at[l], wout.at[l]))
        big.append(part)
    small[0].start()

    power = n_z & (n_z - 1) == 0
    peers_y = [(lax.rem(my_y + j, n_y), j - 1, n_y - j - 1) for j in range(1, n_y)]
    peers_x = [(lax.rem(my_x + j, chips), j - 1, chips - j - 1) for j in range(1, chips)]
    if power:
        peers_z = [(flip_bits(my_z, j), j - 1, j - 1) for j in range(1, n_z)]
    else:
        peers_z = [(lax.rem(my_z + j, n_z), j - 1, n_z - j - 1) for j in range(1, n_z)]
    barrier = pltpu.get_barrier_semaphore()
    for y, _, _ in peers_y:
        pl.semaphore_signal(
            barrier, inc=1, device_id={"tp": my_z * n_y + y}, device_id_type=MESH
        )
    for z, _, _ in peers_z:
        pl.semaphore_signal(
            barrier, inc=1, device_id={"tp": z * n_y + my_y}, device_id_type=MESH
        )
    for x, _, _ in peers_x:
        pl.semaphore_signal(
            barrier, inc=1, device_id={"dp": x * 2 + my_core}, device_id_type=MESH
        )
    pl.semaphore_signal(barrier, inc=1, device_id={"dp": peer}, device_id_type=MESH)
    for copy in small[1:] + big[0] + big[1]:
        copy.start()
    pl.semaphore_wait(barrier, len(peers_y) + len(peers_z) + chips)

    def remote(src, dst, s, rcv, where):
        return pltpu.make_async_remote_copy(
            src_ref=src, dst_ref=dst, send_sem=s, recv_sem=rcv, device_id=where, device_id_type=MESH
        )

    def tp_rows(t):
        return pl.ds(pl.multiple_of(t * own_rows, own_rows), own_rows)

    def x_rows(x):
        return pl.ds(pl.multiple_of(x * rows, rows), rows)

    def drain_sent(ref, sem_ref):
        remote(ref, ref, sem_ref, sem_ref, {"dp": peer}).wait_send()

    def drain_received(ref, sem_ref):
        remote(ref, ref, sem_ref, sem_ref, {"dp": peer}).wait_recv()

    def block_rows(count):
        return pl.ds(0, count * own_rows)

    def gather_z(l, b, peer_z, own=True):
        z, here, there = peer_z
        return remote(
            current.at[l, b],
            gathered.at[l, b, tp_rows((my_z if own else z) * n_y + my_y)],
            r.gat_s.at[b],
            r.gat_r.at[b, there if own else here],
            {"tp": z * n_y + my_y},
        )

    def gather_y(l, b, z, peer_y, own):
        part = gathered.at[l, b, tp_rows(z * n_y + my_y)]
        return remote(
            current.at[l, b] if own else part,
            part,
            r.gat_s.at[b] if own else r.gfw_s.at[b],
            r.gfw_r.at[b],
            {"tp": my_z * n_y + peer_y[0]},
        )

    def one_gate(l, b):
        return remote(
            r.send1g.at[l, b],
            r.recv1g.at[l, b],
            r.one_s.at[b, 1],
            r.one_r.at[b, 4],
            {"dp": peer},
        )

    def one_main(l, b, c):
        return remote(
            r.send1.at[l, b, c],
            r.recv1.at[l, b, c],
            r.one_s.at[b, 0],
            r.one_r.at[b, c],
            {"dp": peer},
        )

    def two_gate(l, b, peer_x):
        x, _, there = peer_x
        return remote(
            r.send2g.at[l, b, x_rows(x)],
            r.recv2g.at[l, b, there],
            r.two_s.at[b, 1],
            r.two_r.at[b, 1],
            {"dp": x * 2 + my_core},
        )

    def two_main(l, b, c, peer_x):
        x, _, there = peer_x
        return remote(
            r.send2.at[l, b, c, x_rows(x)],
            r.recv2.at[l, b, c, there],
            r.two_s.at[b, 0],
            r.two_r.at[b, 0],
            {"dp": x * 2 + my_core},
        )

    def across(l, b, peer_x, own=True):
        x, here, there = peer_x
        part = gated.at[l, b, my_dp if own else x * 2 + my_core]
        return remote(
            part,
            part,
            r.gg_s.at[b],
            r.gg_r.at[b, there if own else here],
            {"dp": x * 2 + my_core},
        )

    def inside(l, b, block):
        part = gated.at[l, b, block]
        return remote(part, part, r.fw_s.at[b], r.fw_r.at[b], {"dp": peer})

    def scatter_y(l, b, z, peer_y):
        y, _, there = peer_y
        return remote(
            mixed.at[l, b, tp_rows(z * n_y + y)],
            r.mixed_y.at[l, b, z, there],
            r.my_s.at[b],
            r.my_r.at[b, z],
            {"tp": my_z * n_y + y},
        )

    def scatter_z(l, b, peer_z):
        z, here, there = peer_z
        return remote(
            r.mixed_s.at[l, b, here],
            r.mixed_in.at[l, b, there],
            r.mix_s.at[b],
            r.mix_r.at[b],
            {"tp": z * n_y + my_y},
        )

    def sent_gather(l, b):
        drain_sent(gathered.at[l, b, block_rows(n_z + n_y - 2)], r.gat_s.at[b])
        drain_sent(gathered.at[l, b, block_rows((n_z - 1) * (n_y - 1))], r.gfw_s.at[b])

    def sent_project(l, b):
        drain_sent(r.send1.at[l, b], r.one_s.at[b, 0])
        drain_sent(r.send1g.at[l, b], r.one_s.at[b, 1])
        drain_sent(r.recv2.at[l, b], r.two_s.at[b, 0])
        drain_sent(r.recv2g.at[l, b], r.two_s.at[b, 1])

    def sent_attend(l, b):
        drain_sent(gated.at[l, b, pl.ds(0, chips - 1)], r.gg_s.at[b])
        drain_sent(gated.at[l, b, pl.ds(0, chips)], r.fw_s.at[b])

    def sent_mix(l, b):
        drain_sent(r.mixed_y.at[l, b], r.my_s.at[b])
        drain_sent(r.mixed_s.at[l, b], r.mix_s.at[b])

    def begin(l, b):
        if l:
            sent_gather(l - 1, b)
        for peer_z in peers_z:
            gather_z(l, b, peer_z).start()
        for peer_y in peers_y:
            gather_y(l, b, my_z, peer_y, own=True).start()
        gathered[l, b, tp_rows(my_tp)] = current[l, b]

    small[0].wait()
    for b in range(BATCHES):
        begin(0, b)
    for copy in small[1:]:
        copy.wait()

    row_id = lax.broadcasted_iota(jnp.int32, (rows, rows), 0)
    col_id = lax.broadcasted_iota(jnp.int32, (rows, rows), 1)
    allowed = (row_id // span == col_id // span) & (col_id <= row_id)
    lane = lax.broadcasted_iota(jnp.int32, (rows, LANES), 1)
    row_l = lax.broadcasted_iota(jnp.int32, (rows, LANES), 0)
    runs = [
        [slice(j * own_seqs + b * own_part, j * own_seqs + (b + 1) * own_part) for j in range(ratio)]
        for b in range(BATCHES)
    ]

    def live_of(b):
        reach = jnp.zeros((rows, LANES), jnp.int32)
        place = 0
        for run in runs[b]:
            for s in range(run.start, run.stop):
                reach = jnp.where(row_l // span == place, lengths[s], reach)
                place = place + 1
        return lax.rem(row_l, span) < reach

    pad[...] = jnp.zeros_like(pad)
    for l in range(LAYERS):
        pad[l, 0:seqs, 0:heads] = jnp.transpose(stabils[l])
        pad[l, seqs : seqs + 1, 0:heads] = r.bias[l : l + 1, :]

    def spread(value):
        wide = jnp.broadcast_to(value[:, None, :], (seqs_b, span, value.shape[-1]))
        return wide.reshape(rows, value.shape[-1])

    def last(value):
        return value.reshape(seqs_b, span, value.shape[-1])[:, span - 1, :]

    arrived = set()

    def arrive(l, first, end):
        if (l, first) not in arrived:
            arrived.add((l, first))
            if end == first + 1:
                big[l][first].wait()
            else:
                whole = wgate.at[l] if first == 0 else wts.at[l]
                load(6 + 4 * l + (first > 0), whole, whole).wait()

    def gate_columns(l):
        arrive(l, 0, 2)
        total_heads = wgate.shape[2]
        pick_r = lax.broadcasted_iota(jnp.int32, (LANES, total_heads), 1)
        pick_c = lax.broadcasted_iota(jnp.int32, (LANES, total_heads), 0)
        head_start = my_tp * heads
        pick_in = ((pick_r == head_start + pick_c) & (pick_c < heads)).astype(F32).astype(BF16)
        pick_fg = (
            ((pick_r == head_start + pick_c - heads) & (pick_c >= heads) & (pick_c < 2 * heads))
            .astype(F32)
            .astype(BF16)
        )
        gate_w[l] = (
            jnp.dot(pick_in, wgate[l, 0], preferred_element_type=F32)
            + jnp.dot(pick_fg, wgate[l, 1], preferred_element_type=F32)
        ).astype(BF16)

    for l in range(LAYERS):
        gate_columns(l)

    def forward(l, b, j):
        gather_z(l, b, peers_z[j], own=False).wait_recv()
        for peer_y in peers_y:
            gather_y(l, b, peers_z[j][0], peer_y, own=False).start()

    def project(l, b):
        if l:
            sent_project(l - 1, b)
        drain_received(gathered.at[l, b, block_rows(n_z * (n_y - 1))], r.gfw_r.at[b])
        gain_row = gain[l : l + 1, :]
        for d in range(n_dp):
            block = gathered[l, b, d * rows : (d + 1) * rows].astype(F32)
            core, x = d % 2, d // 2
            role = lax.rem(my_core + core, 2)
            scaled[role, x * rows : (x + 1) * rows] = (block * gain_row).astype(BF16)
            own_gate[b, role, x * rows : (x + 1) * rows] = jnp.broadcast_to(
                jnp.sum(block * block, axis=1, keepdims=True), (rows, LANES)
            )
        lane_all = lax.broadcasted_iota(jnp.int32, (chips * rows, LANES), 1)
        part = lax.dot_general(
            scaled[...].reshape(2 * chips * rows, feat),
            gate_w[l],
            (((1,), (1,)), ((), ())),
            preferred_element_type=F32,
        ).reshape(2, chips * rows, LANES)
        for role in range(2):
            own_gate[b, role] = jnp.where(lane_all == LANES - 3, own_gate[b, role], part[role])
        r.send1g[l, b] = pack_squares(own_gate[b, 1])
        one_gate(l, b).start()
        arrive(l, 2, 6)

        def one(c, carry):
            flat = scaled[...].reshape(2 * chips * rows, feat)
            both = jnp.dot(flat, wts[l, c], preferred_element_type=F32)
            r.send1[l, b, c] = both[chips * rows :].astype(BF16)
            one_main(l, b, c).start()
            own_main[b, c] = both[: chips * rows]

            @pl.when(c == AHEAD)
            def _():
                exchange_gate(l, b)

            @pl.when(c >= AHEAD)
            def _():
                exchange_main(l, b, c - AHEAD)

            return carry

        lax.fori_loop(0, 4, one, 0)

    def exchange_gate(l, b):
        one_gate(l, b).wait_recv()
        summed = own_gate[b, 0] + r.recv1g[l, b].astype(F32)
        own_gate[b, 0] = summed
        r.send2g[l, b] = pack_squares(summed)
        for peer_x in peers_x:
            two_gate(l, b, peer_x).start()

    def exchange_main(l, b, c):
        one_main(l, b, c).wait_recv()
        own = own_main[b, c] + r.recv1[l, b, c].astype(F32)
        own_main[b, c] = own
        r.send2[l, b, c] = own.astype(BF16)
        for peer_x in peers_x:
            two_main(l, b, c, peer_x).start()

    def exchange(l, b):
        def one(c, carry):
            exchange_main(l, b, c)
            return carry

        lax.fori_loop(4 - AHEAD, 4, one, 0)

    before, kept = {}, {}

    def gates(l, b):
        live = live_of(b)
        drain_received(r.recv2g.at[l, b], r.two_r.at[b, 1])
        sums = own_gate[b, 0, x_rows(my_x)]
        for j in range(chips - 1):
            sums = sums + r.recv2g[l, b, j].astype(F32)
        square = jnp.sum(jnp.where(lane >= LANES - 3, sums, 0.0), axis=1, keepdims=True)
        scale = lax.rsqrt(square / (feat * n_dp) + EPSILON)
        pre = scale * sums
        stabil = jnp.concatenate([pad[l, run] for run in runs[b]], axis=0)
        forget = pltpu.roll(pre, LANES - heads, 1) + pad[l, seqs : seqs + 1, :]
        log_forget = jnp.minimum(forget, 0.0) - jnp.log1p(jnp.exp(-jnp.abs(forget)))
        in_gate = jnp.where(live, pre, NEG_FILL)
        log_forget = jnp.where(live, log_forget, 0.0)
        cumul = jnp.dot(
            allowed.astype(F32), log_forget, preferred_element_type=F32, precision=HIGH
        )
        carried = cumul + spread(stabil)
        source = jnp.transpose(in_gate - cumul)
        before[l, b] = live, scale, stabil, in_gate, cumul, carried, source

    def attend(l, b):
        live, scale, stabil, in_gate, cumul, carried, source = before[l, b]
        if l:
            sent_attend(l - 1, b)
        arrive(l, 6, 7)
        drain_received(r.recv2.at[l, b], r.two_r.at[b, 0])
        for c in range(4):
            full = own_main[b, c, x_rows(my_x)]
            for j in range(chips - 1):
                full = full + r.recv2[l, b, c, j].astype(F32)
            heads_buf[l, b, c] = (scale * full).astype(BF16)

        ids = [s for run in runs[b] for s in range(run.start, run.stop)]
        running = jnp.zeros((rows, LANES), F32)
        for h in range(heads):
            span_h = slice(h * size, (h + 1) * size)
            normer = jnp.concatenate([norm[l, run, h, :] for run in runs[b]], axis=0)
            q, k, v = (heads_buf[l, b, c, :, span_h] for c in range(3))
            weight = jnp.where(allowed, cumul[:, h : h + 1] + source[h : h + 1, :], NEG_FILL)
            top = jnp.maximum(jnp.max(weight, axis=1, keepdims=True), carried[:, h : h + 1])
            running = jnp.where(lane == h, top, running)
            decay = jnp.exp(carried[:, h : h + 1] - top)
            scores = lax.dot_general(
                q, k, (((1,), (1,)), ((), ())), preferred_element_type=F32
            )
            scores = scores * key_scale * jnp.exp(weight - top)
            numer = jnp.dot(scores.astype(BF16), v, preferred_element_type=F32)
            from_cell = jnp.concatenate(
                [
                    jnp.dot(
                        q[i * span : (i + 1) * span],
                        cells[l, s, h].astype(BF16),
                        preferred_element_type=F32,
                    )
                    for i, s in enumerate(ids)
                ],
                axis=0,
            )
            numer = numer + decay * from_cell
            from_norm = jnp.sum(q.astype(F32) * spread(normer), axis=1, keepdims=True)
            denom = jnp.sum(scores, axis=1, keepdims=True) + decay * from_norm
            readout = numer / jnp.maximum(jnp.abs(denom), 1.0)
            readout = jnp.where(live, readout, 0.0)
            outgate = heads_buf[l, b, 3, :, span_h].astype(F32)
            gated[l, b, my_dp, :, span_h] = (readout / (1.0 + jnp.exp(-outgate))).astype(BF16)

        for peer_x in peers_x:
            across(l, b, peer_x).start()
        inside(l, b, my_dp).start()
        kept[l, b] = running, cumul, in_gate, stabil

    def update(l, b):
        running, cumul, in_gate, stabil = kept[l, b]
        ids = [s for run in runs[b] for s in range(run.start, run.stop)]
        top_last, cumul_last = last(running), last(cumul)
        weights = jnp.exp(spread(cumul_last - top_last) - cumul + in_gate)
        fade = jnp.exp(cumul_last + stabil - top_last)
        for j, run in enumerate(runs[b]):
            top_buf[l, run] = top_last[j * own_part : (j + 1) * own_part]
        seq_col = lax.broadcasted_iota(jnp.int32, (size, rows), 1) // span
        pick = (
            lax.broadcasted_iota(jnp.int32, (seqs_b, rows), 1) // span
            == lax.broadcasted_iota(jnp.int32, (seqs_b, rows), 0)
        ).astype(F32)
        for h in range(heads):
            span_h = slice(h * size, (h + 1) * size)
            normer = jnp.concatenate([norm[l, run, h, :] for run in runs[b]], axis=0)
            v = heads_buf[l, b, 2, :, span_h]
            k = heads_buf[l, b, 1, :, span_h].astype(F32) * key_scale * weights[:, h : h + 1]
            flipped = jnp.transpose(k)
            stacked = jnp.concatenate(
                [jnp.where(seq_col == i, flipped, 0.0).astype(BF16) for i in range(seqs_b)], axis=0
            )
            added = jnp.dot(stacked, v, preferred_element_type=F32)
            for i, s in enumerate(ids):
                cells[l, s, h] = (
                    fade[i : i + 1, h : h + 1] * cells[l, s, h]
                    + added[i * size : (i + 1) * size]
                )
            moved = fade[:, h : h + 1] * normer + jnp.dot(
                pick, k, preferred_element_type=F32, precision=HIGH
            )
            for j, run in enumerate(runs[b]):
                norm_out[l, run, h, :] = moved[j * own_part : (j + 1) * own_part]

    def relay(l, b):
        for peer_x in peers_x:
            across(l, b, peer_x, own=False).wait_recv()
            inside(l, b, peer_x[0] * 2 + my_core).start()

    def mix(l, b):
        arrive(l, 7, 8)
        if l:
            sent_mix(l - 1, b)
        drain_received(gated.at[l, b, pl.ds(0, chips)], r.fw_r.at[b])
        flat = gated[l, b].reshape(total_rows, heads * size)
        mixed[l, b] = jnp.dot(flat, wout[l], preferred_element_type=F32).astype(BF16)
        for z in [peer_z[0] for peer_z in peers_z[::-1]] + [my_z]:
            for peer_y in peers_y:
                scatter_y(l, b, z, peer_y).start()

    def folded(l, b, z):
        total = mixed[l, b, tp_rows(z * n_y + my_y), :].astype(F32)
        drain_received(r.mixed_y.at[l, b, z], r.my_r.at[b, z])
        for j in range(n_y - 1):
            total = total + r.mixed_y[l, b, z, j].astype(F32)
        return total

    def fold(l, b, j):
        peer_z = peers_z[::-1][j]
        r.mixed_s[l, b, peer_z[1]] = folded(l, b, peer_z[0]).astype(BF16)
        scatter_z(l, b, peer_z).start()

    def finish(l, b):
        total = folded(l, b, my_z)
        drain_received(r.mixed_in.at[l, b], r.mix_r.at[b])
        for j in range(n_z - 1):
            total = total + r.mixed_in[l, b, j].astype(F32)
        result = (current[l, b].astype(F32) + total).astype(BF16)
        if l == LAYERS - 1:
            tokens_out[b] = result
        else:
            current[l + 1, b] = result
            begin(l + 1, b)

    steps = (forward, project, exchange, attend, update, relay, mix, fold, finish, gates)
    for l, b, step, j in plan(n_z):
        if step in (FORWARD, FOLD):
            steps[step](l, b, j)
        else:
            steps[step](l, b)

    for l in range(LAYERS):
        max_out[l] = jnp.transpose(top_buf[l])[0:heads, :]
    for b in range(BATCHES):
        for sent in (sent_gather, sent_project, sent_attend, sent_mix):
            sent(LAYERS - 1, b)


def store(*refs):
    sem = refs[-1]
    copies = [pltpu.make_async_copy(refs[i], refs[4 + i], sem.at[i]) for i in range(4)]
    for copy in copies:
        copy.start()
    for copy in copies:
        copy.wait()


def per_device(
    tokens,
    lengths,
    norm_gain,
    query_weight,
    key_weight,
    value_weight,
    outgate_weight,
    input_gate_weight,
    forget_gate_weight,
    forget_bias,
    out_weight,
    cell_state,
    norm_state,
    max_state,
):
    n_tp, n_dp = lax.axis_size("tp"), lax.axis_size("dp")
    seq_here, span, feat = tokens.shape
    seqs, heads, size = cell_state.shape[1:4]
    own_rows, rows = seq_here * span // BATCHES, seqs * span // BATCHES
    cols, chips = heads * size, n_dp // 2
    everyone, many = n_tp * own_rows, chips * rows
    n_y = chips if n_tp % chips == 0 else 1
    n_z = n_tp // n_y
    vmem = pl.BlockSpec(memory_space=pltpu.VMEM)
    hbm = pl.BlockSpec(memory_space=pltpu.HBM)
    V, sem = pltpu.VMEM, pltpu.SemaphoreType.DMA
    LB = (LAYERS, BATCHES)
    inputs = dict(
        tokens=tokens.reshape(BATCHES, own_rows, feat),
        lengths_in=lengths,
        gain_in=norm_gain,
        weight_q=query_weight,
        weight_k=key_weight,
        weight_v=value_weight,
        weight_o=outgate_weight,
        weight_in=jnp.swapaxes(input_gate_weight, 1, 2),
        weight_forget=jnp.swapaxes(forget_gate_weight, 1, 2),
        bias_in=forget_bias,
        weight_out=out_weight,
        cell_in=cell_state,
        norm_in=norm_state,
        max_in=jnp.swapaxes(max_state, 1, 2),
    )
    outputs = dict(
        tokens_out=V((BATCHES, own_rows, feat), BF16),
        cells=V(cell_state.shape, F32),
        norm_out=V(norm_state.shape, F32),
        max_out=V((LAYERS, heads, seqs), F32),
    )
    scratch = dict(
        lengths=pltpu.SMEM(lengths.shape, jnp.int32),
        gain=V(norm_gain.shape, F32),
        norm=V(norm_state.shape, F32),
        stabils=V((LAYERS, heads, seqs), F32),
        bias=V(forget_bias.shape, F32),
        current=V((*LB, own_rows, feat), BF16),
        wts=V((LAYERS, 4, feat, cols), BF16),
        wgate=V((LAYERS, 2, input_gate_weight.shape[2], feat), BF16),
        wout=V((LAYERS, cols, feat), BF16),
        pad=V((LAYERS, seqs + 8, LANES), F32),
        top_buf=V((LAYERS, seqs, LANES), F32),
        gate_w=V((LAYERS, LANES, feat), BF16),
        gathered=V((*LB, everyone, feat), BF16),
        scaled=V((2, many, feat), BF16),
        own_main=V((BATCHES, 4, many, cols), F32),
        own_gate=V((BATCHES, 2, many, LANES), F32),
        send1=V((*LB, 4, many, cols), BF16),
        send1g=V((*LB, many, LANES), BF16),
        recv1=V((*LB, 4, many, cols), BF16),
        recv1g=V((*LB, many, LANES), BF16),
        send2=V((*LB, 4, many, cols), BF16),
        send2g=V((*LB, many, LANES), BF16),
        recv2=V((*LB, 4, chips - 1, rows, cols), BF16),
        recv2g=V((*LB, chips - 1, rows, LANES), BF16),
        heads_buf=V((*LB, 4, rows, cols), BF16),
        gated=V((*LB, n_dp, rows, cols), BF16),
        mixed=V((*LB, everyone, feat), BF16),
        mixed_s=V((*LB, n_z - 1, own_rows, feat), BF16),
        mixed_y=V((*LB, n_z, n_y - 1, own_rows, feat), BF16),
        mixed_in=V((*LB, n_z - 1, own_rows, feat), BF16),
        load_sem=sem((6 + 4 * LAYERS,)),
        gat_s=sem((BATCHES,)),
        gat_r=sem((BATCHES, n_z - 1)),
        gfw_s=sem((BATCHES,)),
        gfw_r=sem((BATCHES,)),
        one_s=sem((BATCHES, 2)),
        one_r=sem((BATCHES, 5)),
        two_s=sem((BATCHES, 2)),
        two_r=sem((BATCHES, 2)),
        gg_s=sem((BATCHES,)),
        gg_r=sem((BATCHES, chips - 1)),
        fw_s=sem((BATCHES,)),
        fw_r=sem((BATCHES,)),
        mix_s=sem((BATCHES,)),
        mix_r=sem((BATCHES,)),
        my_s=sem((BATCHES,)),
        my_r=sem((BATCHES, n_z)),
    )
    names = (*inputs, *outputs, *scratch)
    result = pl.pallas_call(
        functools.partial(kernel, (n_tp, n_dp, span, heads, size, n_y, names)),
        out_shape=tuple(outputs.values()),
        in_specs=[hbm] * len(inputs),
        out_specs=(vmem,) * len(outputs),
        scratch_shapes=list(scratch.values()),
        compiler_params=pltpu.CompilerParams(
            collective_id=0, has_side_effects=True, vmem_limit_bytes=56 * 1024 * 1024
        ),
    )(*inputs.values())
    result = pl.pallas_call(
        store,
        out_shape=tuple(jax.ShapeDtypeStruct(part.shape, part.dtype) for part in result),
        in_specs=[vmem] * 4,
        out_specs=(pl.BlockSpec(memory_space=pl.ANY),) * 4,
        scratch_shapes=[sem((4,))],
        compiler_params=pltpu.CompilerParams(vmem_limit_bytes=16 * 1024 * 1024),
    )(*result)
    return (result[0].reshape(tokens.shape), *result[1:3], jnp.swapaxes(result[3], 1, 2))


def solution(mesh):
    return jax.shard_map(
        per_device,
        mesh=mesh,
        in_specs=(
            P("tp", None, "dp"),
            P("dp"),
            P(None, "dp"),
            P(None, "dp", "tp"),
            P(None, "dp", "tp"),
            P(None, "dp", "tp"),
            P(None, "dp", "tp"),
            P(),
            P(),
            P(None, "tp"),
            P(None, "tp", "dp"),
            P(None, "dp", "tp", None, None),
            P(None, "dp", "tp", None),
            P(None, "dp", "tp"),
        ),
        out_specs=(
            P("tp", None, "dp"),
            P(None, "dp", "tp", None, None),
            P(None, "dp", "tp", None),
            P(None, "dp", "tp"),
        ),
        check_vma=False,
    )
```
